32 devices in a mesh: sp: 8 (over z, x), tp: 4 (over y, core).
Axes of the slice: x: 2, y: 2, z: 4, core: 2. Of those that a mesh axis runs over, the one named last changes fastest.
Arguments:
- x_res: bfloat16 [2048, 2048], P(('sp', 'tp')), may hold values from -6 to 6
- q_a: bfloat16 [2048, 1024], P('sp', 'tp'), may hold values from -48 to 48
- k_a: bfloat16 [2048, 256], P('sp', 'tp'), may hold values from -48 to 48
- v_a: bfloat16 [2048, 256], P('sp', 'tp'), may hold values from -6 to 6
- q_b: bfloat16 [2048, 1024], P('sp', 'tp'), may hold values from -48 to 48
- k_b: bfloat16 [2048, 512], P('sp', 'tp'), may hold values from -48 to 48
- v_b: bfloat16 [2048, 512], P('sp', 'tp'), may hold values from -6 to 6
- gain_qa: float32 [64], replicated, may hold values from 1.2 to 6
- gain_ka: float32 [64], replicated, may hold values from 1.2 to 6
- gain_qb: float32 [128], replicated, may hold values from 1.2 to 6
- gain_kb: float32 [128], replicated, may hold values from 1.2 to 6
- w_out_a: bfloat16 [1024, 2048], P('tp'), may hold values from -0.125 to 0.125
- w_out_b: bfloat16 [1024, 2048], P('tp'), may hold values from -0.125 to 0.125
- gain_mid: float32 [2048], replicated, may hold values from 0.1 to 1.9
- w_gate: bfloat16 [2048, 3072], P('sp', 'tp'), may hold values from -0.125 to 0.125
- w_up: bfloat16 [2048, 3072], P('sp', 'tp'), may hold values from -0.125 to 0.125
- conv_gate: float32 [3, 3072], P(None, 'tp'), may hold values from -3.5 to 3.5
- conv_up: float32 [3, 3072], P(None, 'tp'), may hold values from -3.5 to 3.5
- w_down: bfloat16 [3072, 2048], P('tp', 'sp'), may hold values from -0.109375 to 0.109375
Outputs:
- layer_out: bfloat16 [2048, 2048], P(('sp', 'tp'))
The draws below stay inside these ranges and needn't reach their ends.
All inputs are finite; a program needn't handle non-finite values.
Results may differ from the reference program's by a relative error of at most 0.014.
The reference program's roundings to bfloat16 on the way (of `qa_n`, `ka_n`, `qb_n`, `kb_n`, `normed`, `gate_pre`, `up_pre` and `hidden`) count: a program that leaves them out, or rounds other values in their place, can miss the bound.
Values may be sent and summed in bfloat16 or wider, within the bound.
A program may use at most 128 MiB of HBM per device.

```python
import jax
import jax.numpy as jnp
from jax import lax

D = 2048
FF = 3072
HQA = 16
HKVA = 4
DHA = 64
HQB = 8
HKVB = 4
DHB = 128
TOKENS = 2048
N_TP = 4


def drawn_keys(key, heads, head_size, salt):
    base = jax.random.fold_in(key, salt)
    streams = jax.random.split(base, 1)
    keys = jax.random.truncated_normal(streams[0], -4.0, 4.0, (TOKENS, heads, head_size), jnp.float32)
    return keys


def drawn_queries(key, heads, head_size, salt):
    queries = jax.random.truncated_normal(jax.random.fold_in(key, salt + 1), -4.0, 4.0, (TOKENS, heads, head_size), jnp.float32)
    return queries.reshape(TOKENS, heads * head_size).astype(jnp.bfloat16)


def drawn_gain(key, head_size, salt):
    gains = jax.random.uniform(jax.random.fold_in(key, salt), (head_size,), jnp.float32, 1.2, 2.4)
    return gains


def draw_q_a(key, part):
    return drawn_queries(key, HQA, DHA, 11)


def draw_k_a(key, part):
    keys = drawn_keys(key, HKVA, DHA, 11)
    return keys.reshape(TOKENS, HKVA * DHA).astype(jnp.bfloat16)


def draw_q_b(key, part):
    return drawn_queries(key, HQB, DHB, 21)


def draw_k_b(key, part):
    keys = drawn_keys(key, HKVB, DHB, 21)
    return keys.reshape(TOKENS, HKVB * DHB).astype(jnp.bfloat16)


def draw_gain_qa(key, part):
    return drawn_gain(key, DHA, 31)


def draw_gain_ka(key, part):
    return drawn_gain(key, DHA, 32)


def draw_gain_qb(key, part):
    return drawn_gain(key, DHB, 33)


def draw_gain_kb(key, part):
    return drawn_gain(key, DHB, 34)


def steps_of(rng, extent, pieces, low, top_value):
    def one(axis_at, blocks):
        heights = jax.random.uniform(jax.random.fold_in(jax.random.fold_in(rng, 6), axis_at), (blocks,), jnp.float32, low / len(pieces), top_value / len(pieces))
        return jnp.repeat(jnp.exp(heights), extent[axis_at] // blocks).reshape((-1,) + (1,) * (len(extent) - axis_at - 1))

    level = one(*pieces[0])
    for cut in pieces[1:]:
        level = level * one(*cut)
    return level


def noise(rng, extent, deviation, bound, cuts=(), held_as=jnp.bfloat16):
    level = steps_of(rng, extent, cuts, -0.22, 0.18) if cuts else 1.0
    values = jax.random.normal(rng, extent, jnp.float32) * deviation * level
    return jnp.minimum(jnp.maximum(values, -bound), bound).astype(held_as)


def setup_inputs(seed: int = 0) -> dict:
    streams_of = jax.random.split(jax.random.key(seed), 20)
    return {
        "x_res": noise(streams_of[0], (TOKENS, D), 1.0, 6.0, ((0, 32),)),
        "q_a": draw_q_a(jax.random.fold_in(streams_of[19], 71), 0),
        "k_a": draw_k_a(jax.random.fold_in(streams_of[19], 71), 0),
        "v_a": noise(streams_of[3], (TOKENS, HKVA * DHA), 1.0, 6.0, ((0, 8), (1, 4))),
        "q_b": draw_q_b(jax.random.fold_in(streams_of[19], 71), 0),
        "k_b": draw_k_b(jax.random.fold_in(streams_of[19], 71), 0),
        "v_b": noise(streams_of[6], (TOKENS, HKVB * DHB), 1.0, 6.0, ((0, 8), (1, 4))),
        "gain_qa": draw_gain_qa(jax.random.fold_in(streams_of[19], 71), 0),
        "gain_ka": draw_gain_ka(jax.random.fold_in(streams_of[19], 71), 0),
        "gain_qb": draw_gain_qb(jax.random.fold_in(streams_of[19], 71), 0),
        "gain_kb": draw_gain_kb(jax.random.fold_in(streams_of[19], 71), 0),
        "w_out_a": noise(streams_of[11], (HQA * DHA, D), (HQA * DHA + HQB * DHB) ** -0.5, 0.125, ((0, 4),)),
        "w_out_b": noise(streams_of[12], (HQB * DHB, D), (HQA * DHA + HQB * DHB) ** -0.5, 0.125, ((0, 4),)),
        "gain_mid": jnp.clip(1.0 + 0.18 * jax.random.normal(streams_of[13], (D,), jnp.float32), 0.1, 1.9),
        "w_gate": noise(streams_of[14], (D, FF), D ** -0.5, 0.125, ((0, 8), (1, 4))),
        "w_up": noise(streams_of[15], (D, FF), D ** -0.5, 0.125, ((0, 8), (1, 4))),
        "conv_gate": noise(streams_of[16], (3, FF), 3 ** -0.5, 3.5, ((1, 4),), jnp.float32),
        "conv_up": noise(streams_of[17], (3, FF), 3 ** -0.5, 3.5, ((1, 4),), jnp.float32),
        "w_down": noise(streams_of[18], (FF, D), FF ** -0.5, 0.109375, ((0, 4), (1, 8))),
    }


norm_eps = 1e-06
rope_theta = 10000.0

def rotary_angles(positions, head_size):
    half = head_size // 2
    inverse = jnp.power(jnp.float32(rope_theta), -jnp.arange(0, half, 2, dtype=jnp.float32) / half)
    grid_row = (positions // 64).astype(jnp.float32)[:, None] * inverse[None, :]
    grid_col = (positions % 64).astype(jnp.float32)[:, None] * inverse[None, :]
    angles = jnp.concatenate([grid_row, grid_row, grid_col, grid_col], axis=-1)
    return (jnp.cos(angles), jnp.sin(angles))

def rotate_half(values):
    first, second = jnp.split(values, 2, axis=-1)
    return jnp.concatenate([-second, first], axis=-1)

def prepare(raw, gain, head_size, positions):
    count = raw.shape[0]
    heads = raw.shape[1] // head_size
    values = raw.astype(jnp.float32).reshape(count, heads, head_size)
    values = values * lax.rsqrt(lax.optimization_barrier(jnp.mean(values * values, axis=-1, keepdims=True)) + norm_eps)
    values = values * gain.astype(jnp.float32)
    cosine, sine = rotary_angles(positions, head_size)
    row_part, col_part = jnp.split(values, 2, axis=-1)
    turned = jnp.concatenate([rotate_half(row_part), rotate_half(col_part)], axis=-1)
    values = values * cosine[:, None, :] + turned * sine[:, None, :]
    return values.astype(jnp.bfloat16)

def attention_group(queries, keys, values, head_size):
    count = queries.shape[0]
    kv_heads = keys.shape[1]
    groups = queries.shape[1] // kv_heads
    block = 256 if count % 256 == 0 else 64
    blocked = queries.reshape(count // block, block, kv_heads, groups, head_size)
    keys_f = keys.astype(jnp.float32)
    values_f = values.astype(jnp.float32)
    scale = jnp.float32(head_size ** (-0.5))

    def one_block(query_block):
        scores = jnp.einsum('qkgd,skd->kgqs', query_block.astype(jnp.float32), keys_f) * scale
        top = lax.optimization_barrier(jnp.max(scores, axis=-1, keepdims=True))
        expd = jnp.exp(scores - top)
        totals = lax.optimization_barrier(jnp.sum(expd, axis=-1))
        weights = expd.astype(jnp.bfloat16).astype(jnp.float32)
        summed = jnp.einsum('kgqs,skd->kgqd', weights, values_f) / totals[..., None]
        return jnp.transpose(summed, (2, 0, 1, 3)).reshape(block, kv_heads * groups * head_size).astype(jnp.bfloat16)
    result = lax.map(one_block, blocked)
    return result.reshape(count, kv_heads * groups * head_size)

def reference(x_res, q_a, k_a, v_a, q_b, k_b, v_b, gain_qa, gain_ka, gain_qb, gain_kb, w_out_a, w_out_b, gain_mid, w_gate, w_up, conv_gate, conv_up, w_down):
    count = x_res.shape[0]
    positions = jnp.arange(count, dtype=jnp.int32)
    qa_n = prepare(q_a, gain_qa, DHA, positions)
    ka_n = prepare(k_a, gain_ka, DHA, positions)
    qb_n = prepare(q_b, gain_qb, DHB, positions)
    kb_n = prepare(k_b, gain_kb, DHB, positions)
    va_h = v_a.reshape(count, HKVA, DHA)
    vb_h = v_b.reshape(count, HKVB, DHB)
    attn_a = attention_group(qa_n, ka_n, va_h, DHA)
    attn_b = attention_group(qb_n, kb_n, vb_h, DHB)
    width_a = HQA * DHA // N_TP
    width_b = HQB * DHB // N_TP
    projected = jnp.zeros((count, D), jnp.float32)
    for block in range(N_TP):
        partial_value = jnp.dot(attn_a[:, block * width_a:(block + 1) * width_a], w_out_a[block * width_a:(block + 1) * width_a], preferred_element_type=jnp.float32)
        partial_value = partial_value + jnp.dot(attn_b[:, block * width_b:(block + 1) * width_b], w_out_b[block * width_b:(block + 1) * width_b], preferred_element_type=jnp.float32)
        projected = projected + partial_value.astype(jnp.bfloat16).astype(jnp.float32)
    mid = x_res.astype(jnp.float32) + projected
    normed = mid * lax.rsqrt(lax.optimization_barrier(jnp.mean(mid * mid, axis=-1, keepdims=True)) + norm_eps)
    normed = (normed * gain_mid.astype(jnp.float32)).astype(jnp.bfloat16)
    gate_pre = jnp.dot(normed, w_gate, preferred_element_type=jnp.float32).astype(jnp.bfloat16)
    up_pre = jnp.dot(normed, w_up, preferred_element_type=jnp.float32).astype(jnp.bfloat16)

    def convolve(projected_rows, taps):
        padded = jnp.pad(projected_rows.astype(jnp.float32), ((1, 1), (0, 0)))
        taps = taps.astype(jnp.float32)
        return padded[:-2] * taps[0] + padded[1:-1] * taps[1] + padded[2:] * taps[2]
    gate_conv = convolve(gate_pre, conv_gate)
    up_conv = convolve(up_pre, conv_up)
    hidden = (jax.nn.silu(gate_conv) * up_conv).astype(jnp.bfloat16)
    width_f = FF // N_TP
    down = jnp.zeros((count, D), jnp.float32)
    for block in range(N_TP):
        partial_value = jnp.dot(hidden[:, block * width_f:(block + 1) * width_f], w_down[block * width_f:(block + 1) * width_f], preferred_element_type=jnp.float32)
        down = down + partial_value.astype(jnp.bfloat16).astype(jnp.float32)
    return (mid + down).astype(jnp.bfloat16)
```

```python
import functools

import jax
import jax.numpy as jnp
import numpy as np
from jax import lax
from jax.experimental import pallas as pl
from jax.experimental.pallas import tpu as pltpu
from jax.sharding import PartitionSpec as P

DHA = 64
DHB = 128

norm_eps = 1e-06
rope_theta = 10000.0
F32 = jnp.float32
BF16 = jnp.bfloat16
MESH = pl.DeviceIdType.MESH
GU_PIECES = 4
DN_PIECES = 2


def rotary_angles(positions, head_size):
    half = head_size // 2
    inverse = jnp.power(jnp.float32(rope_theta), -jnp.arange(0, half, 2, dtype=jnp.float32) / half)
    grid_row = (positions // 64).astype(jnp.float32)[:, None] * inverse[None, :]
    grid_col = (positions % 64).astype(jnp.float32)[:, None] * inverse[None, :]
    return jnp.concatenate([grid_row, grid_row, grid_col, grid_col], axis=-1)


def lane_frequencies(head_size, width):
    half = head_size // 2
    steps = -np.arange(0, half, 2, dtype=np.float32) / np.float32(half)
    inverse = np.power(np.float32(rope_theta), steps).astype(np.float32)
    return jnp.asarray(np.tile(inverse, width // inverse.shape[0])[None])


def block_mean(width, head):
    i = lax.broadcasted_iota(jnp.int32, (width, width), 0)
    j = lax.broadcasted_iota(jnp.int32, (width, width), 1)
    return jnp.where(lax.div(i, head) == lax.div(j, head), F32(1.0 / head), F32(0.0))


def block_turn(width, head):
    quarter = head // 4
    i = lax.broadcasted_iota(jnp.int32, (width, width), 0)
    j = lax.broadcasted_iota(jnp.int32, (width, width), 1)
    first = lax.rem(j, 2 * quarter) < quarter
    return jnp.where(
        first & (i == j + quarter),
        F32(-1.0),
        jnp.where(jnp.logical_not(first) & (i == j - quarter), F32(1.0), F32(0.0)),
    )


def exact_dot(a, b):
    return jnp.dot(a, b, precision=lax.Precision.HIGHEST, preferred_element_type=F32)


def prepared(raw, gain, angle_cos, angle_sin, head):
    width = raw.shape[1]
    values = raw.astype(F32)
    values = values * lax.rsqrt(exact_dot(values * values, block_mean(width, head)) + norm_eps)
    values = values * gain
    turned = exact_dot(values, block_turn(width, head))
    return (values * angle_cos + turned * angle_sin).astype(BF16)


def kernel(
    x_ref, qa_ref, kat_ref, vat_ref, qb_ref, kb_ref, vb_ref,
    gqa_ref, gka_ref, gqb_ref, gkb_ref,
    fra_ref, frb_ref,
    woa_hbm, wob_hbm, gmid_ref, wg_hbm, wu_hbm, cg_ref, cu_ref, wd_hbm,
    out_ref,
    kv, qas, qbs, m_a, l_a, acc_a, m_b, l_b, acc_b,
    woa, wob, gub, gux, dnb, dnx,
    attn, pout, own1, s1_in, q1, s2_in, mid, nrm, acc, eg_out, eg_x, eg_p, hid,
    p2, own2, s2a, q2, s2b,
    loc_sem, kvz_s, kvz_r, kvx_s, kvx_r, guz_s, guz_r, gux_s, gux_r,
    dnz_s, dnz_r, dnx_s, dnx_r, s1_s, s1_r, s2_s, s2_r,
    agz_s, agz_r, agy_s, agy_r, agf_s, agf_r, agc_s, agc_r, eg_s, eg_r,
    d1_s, d1_r, d2_s, d2_r,
):
    sp = lax.axis_index("sp")
    tp = lax.axis_index("tp")
    z, x = lax.div(sp, 2), lax.rem(sp, 2)
    y, c = lax.div(tp, 2), lax.rem(tp, 2)
    rows = qa_ref.shape[0]
    own = x_ref.shape[0]
    chunk, ff = gub.shape[2], gub.shape[3] // 2
    flip = lax.div(z, 2)

    def mz(v):
        return (1 - flip) * v + flip * (3 - v)

    u = mz(z)
    inner, end = u == 1, u == 0
    mate = mz(1 - u)
    my_h = lax.rem(z, 2)
    jz = my_h
    h_end, h_in = lax.rem(mz(0), 2), lax.rem(mz(1), 2)
    cross = lax.rem(x + flip, 2)
    far = 2 * (1 - flip) * 2 - 2 + z
    twin = 1 - u
    ranks = [u, twin, 2, 3]

    def tp_at(yy, cc):
        return yy * 2 + cc

    barrier = pltpu.get_barrier_semaphore()
    greet = [
        (None, {"sp": 2 * z + 1 - x}),
        (None, {"tp": tp_at(y, 1 - c)}),
        (None, {"tp": tp_at(1 - y, c)}),
        (None, {"sp": 2 * mate + x}),
        (None, {"sp": 2 * mate + x, "tp": tp_at(1 - y, c)}),
        (inner, {"sp": 2 * mz(2) + x}),
        (cross == 1, {"sp": 2 * far + 1 - x}),
    ]
    for cond, where in greet:
        def signal(where=where):
            pl.semaphore_signal(barrier, inc=1, device_id=where, device_id_type=MESH)
        if cond is None:
            signal()
        else:
            pl.when(cond)(signal)

    loc = []
    for h in range(2):
        cut = pl.ds(h * ff, ff)
        loc.append(pltpu.make_async_copy(
            wg_hbm.at[:, cut], gub.at[z, h, :, pl.ds(0, ff)], loc_sem.at[len(loc)]))
        loc.append(pltpu.make_async_copy(
            wu_hbm.at[:, cut], gub.at[z, h, :, pl.ds(ff, ff)], loc_sem.at[len(loc)]))
    for h in range(2):
        loc.append(pltpu.make_async_copy(
            wd_hbm.at[pl.ds(h * ff, ff)], dnb.at[z, h], loc_sem.at[len(loc)]))
    loc.append(pltpu.make_async_copy(woa_hbm, woa, loc_sem.at[len(loc)]))
    loc.append(pltpu.make_async_copy(wob_hbm, wob, loc_sem.at[len(loc)]))
    for copy in loc:
        copy.start()

    def remote(src, dst, send, recv, **where):
        return pltpu.make_async_remote_copy(
            src_ref=src, dst_ref=dst, send_sem=send, recv_sem=recv,
            device_id=where, device_id_type=MESH,
        )

    sent = []

    def under(cond, run):
        if cond is None:
            run()
        else:
            pl.when(cond)(run)

    def go(cond, copies):
        def run():
            for copy in copies:
                copy().start()
        under(cond, run)
        sent.append((cond, copies))

    def got(cond, copies):
        def run():
            for copy in copies:
                copy().wait_recv()
        under(cond, run)

    P = functools.partial
    gr, dr = chunk // GU_PIECES, ff // DN_PIECES
    everyp, everyd = range(GU_PIECES), range(DN_PIECES)

    def kv_z(vb, to, way):
        zi = mz(vb)
        return remote(kv.at[0, zi], kv.at[0, zi], kvz_s.at[way, zi], kvz_r.at[zi], sp=2 * mz(to) + x)

    def kv_x(vb):
        zi = mz(vb)
        return remote(kv.at[0, zi], kv.at[1, zi], kvx_s.at[zi], kvx_r.at[zi], sp=2 * z + 1 - x)

    def gu_z(vb, h, p, to, way):
        zi, cut = mz(vb), pl.ds(p * gr, gr)
        return remote(
            gub.at[zi, h, cut], gub.at[zi, h, cut],
            guz_s.at[way, zi, h, p], guz_r.at[zi, h, p], sp=2 * mz(to) + x,
        )

    def gu_x(vb, p):
        zi, cut = mz(vb), pl.ds(p * gr, gr)
        return remote(
            gub.at[zi, my_h, cut], gux.at[zi, cut],
            gux_s.at[zi, p], gux_r.at[zi, p], sp=2 * z + 1 - x,
        )

    def dn_z(vb, h, p, to, way):
        zi, cut = mz(vb), pl.ds(p * dr, dr)
        return remote(
            dnb.at[zi, h, cut], dnb.at[zi, h, cut],
            dnz_s.at[way, zi, h, p], dnz_r.at[zi, h, p], sp=2 * mz(to) + x,
        )

    def dn_x(vb, p):
        zi, cut = mz(vb), pl.ds(p * dr, dr)
        return remote(
            dnb.at[zi, my_h, cut], dnx.at[zi, cut],
            dnx_s.at[zi, p], dnx_r.at[zi, p], sp=2 * z + 1 - x,
        )

    def gu_to(vb, h, to, way, pieces=everyp):
        return [P(gu_z, vb, h, p, to, way) for p in pieces]

    def dn_to(vb, h, to, way):
        return [P(dn_z, vb, h, p, to, way) for p in everyd]

    def gu_over(vb, pieces=everyp):
        return [P(gu_x, vb, p) for p in pieces]

    def dn_over(vb):
        return [P(dn_x, vb, p) for p in everyd]

    def gu_in(vb, h):
        return [P(gu_z, vb, h, p, 1 - u, 0) for p in everyp]

    def dn_in(vb, h):
        return [P(dn_z, vb, h, p, 1 - u, 0) for p in everyd]

    def kv_in(vb):
        return [P(kv_z, vb, 1 - u, 0)]

    for copy in loc[:4]:
        copy.wait()
    pl.semaphore_wait(barrier, 5 + u + cross)
    go(inner, gu_to(u, h_in, 2, 0, [0]))
    go(inner, gu_to(u, h_end, 0, 1, [0]))
    go(end, gu_to(u, h_in, 1, 0, [0]))
    go(None, gu_over(u, [0]))

    def tables(freq_ref, head):
        shape = (rows, freq_ref.shape[1])
        token = lax.broadcasted_iota(jnp.int32, shape, 0) + sp * rows
        lane = lax.broadcasted_iota(jnp.int32, shape, 1)
        grid = jnp.where(lax.rem(lane, head) < head // 2, lax.div(token, 64), lax.rem(token, 64))
        angles = grid.astype(F32) * freq_ref[...]
        return jnp.cos(angles), jnp.sin(angles)

    ca, sa = tables(fra_ref, DHA)
    cb, sb = tables(frb_ref, DHB)
    wka, wkb = kat_ref.shape[0], kb_ref.shape[1]

    def wide(table, width):
        if width <= table.shape[1]:
            return table[:, :width]
        return jnp.concatenate([table] * (width // table.shape[1]), axis=1)

    def gains(ref, width):
        g = ref[...]
        count = width // g.shape[1]
        return g if count == 1 else jnp.concatenate([g] * count, axis=1)

    raw_a = jnp.transpose(kat_ref[...].astype(F32))
    val_a = jnp.transpose(vat_ref[...].astype(F32)).astype(BF16)
    keys_a = prepared(raw_a, gains(gka_ref, wka), wide(ca, wka), wide(sa, wka), DHA)
    keys_b = prepared(kb_ref[...], gains(gkb_ref, wkb), wide(cb, wkb), wide(sb, wkb), DHB)
    kv[0, z, :, :wkb] = keys_b
    kv[0, z, :, wkb:2 * wkb] = vb_ref[...]
    kv[0, z, :, 2 * wkb:] = jnp.concatenate([keys_a, val_a], axis=1)

    go(inner, [P(kv_z, u, 2, 0), P(kv_z, u, 0, 1)])
    go(end, [P(kv_z, u, 1, 0)])
    go(None, [P(kv_x, u)])
    go(inner, gu_to(u, h_in, 2, 0, [1]) + gu_to(u, h_end, 0, 1, [1]))
    go(end, gu_to(u, h_in, 1, 0, everyp[1:]) + gu_to(u, h_end, 1, 0))
    go(None, gu_over(u, [1]))
    for copy in loc[4:]:
        copy.wait()
    go(end, dn_to(u, h_in, 1, 0) + dn_to(u, h_end, 1, 0))

    heads_a = qa_ref.shape[1] // DHA
    heads_b = qb_ref.shape[1] // DHB
    qa = prepared(
        qa_ref[...], gains(gqa_ref, heads_a * DHA), wide(ca, heads_a * DHA),
        wide(sa, heads_a * DHA), DHA,
    )
    qb = prepared(
        qb_ref[...], gains(gqb_ref, heads_b * DHB), wide(cb, heads_b * DHB),
        wide(sb, heads_b * DHB), DHB,
    )
    for h in range(heads_a):
        qas[h] = qa[:, h * DHA:(h + 1) * DHA]
    for h in range(heads_b):
        qbs[h] = qb[:, h * DHB:(h + 1) * DHB]
    for ref, low in ((m_a, -1e30), (m_b, -1e30), (l_a, 0.0), (l_b, 0.0), (acc_a, 0.0), (acc_b, 0.0)):
        ref[...] = jnp.full(ref.shape, low, F32)

    def attend_one(queries, key_rows, value_rows, m, l, total, h):
        scale = F32(queries.shape[2] ** (-0.5))
        scores = lax.dot_general(
            queries[h], key_rows, (((1,), (1,)), ((), ())), preferred_element_type=F32
        ) * scale
        before = m[h]
        highest = jnp.maximum(before, jnp.max(scores, axis=-1, keepdims=True))
        factor = jnp.exp(before - highest)
        expd = jnp.exp(scores - highest)
        l[h] = l[h] * factor + jnp.sum(expd, axis=-1, keepdims=True)
        total[h] = total[h] * factor + jnp.dot(
            expd.astype(BF16), value_rows, preferred_element_type=F32
        )
        m[h] = highest

    def attend(col, zi):
        for h in range(heads_b):
            attend_one(
                qbs, kv[col, zi, :, :wkb], kv[col, zi, :, wkb:2 * wkb], m_b, l_b, acc_b, h
            )
        pair = kv[col, zi, :, 2 * wkb:]
        for h in range(heads_a):
            attend_one(qas, pair[:, :wka], pair[:, wka:], m_a, l_a, acc_a, h)

    def rank(k):
        high = k // 2 if isinstance(k, int) else lax.div(k, 2)
        return mz(high * k + (1 - high) * (k + u - 2 * k * u))

    attend(0, z)

    def kv_crossed(zi):
        remote(
            kv.at[0, zi], kv.at[1, zi], kvx_s.at[zi], kvx_r.at[zi], sp=2 * z + 1 - x
        ).wait_recv()

    def attend_step(i, carry):
        @pl.when(i == 1)
        def _():
            got(None, kv_in(twin))
            go(inner, [P(kv_z, 0, 2, 0)])
            go(None, [P(kv_x, twin)])
            got(inner, kv_in(2))
            go(inner, [P(kv_z, 2, 0, 1), P(kv_x, 2)])
            go(inner, gu_to(u, h_in, 2, 0, everyp[2:]) + gu_to(u, h_end, 2, 0))
            go(inner, gu_to(u, h_end, 0, 1, [2]))
            go(end, gu_over(u, [2]))

        @pl.when(i == 2)
        def _():
            got(end, kv_in(2))
            go(end, [P(kv_x, 2)])
            got(inner, kv_in(3))
            go(inner, [P(kv_z, 3, 0, 1), P(kv_x, 3)])
            go(inner, gu_to(u, h_end, 0, 1, everyp[3:]))
            go(inner, gu_over(u, [2]))

        @pl.when(i == 3)
        def _():
            got(end, kv_in(3))
            go(end, [P(kv_x, 3)])
            go(None, gu_over(u, everyp[3:]))
            got(inner, gu_in(2, h_end))
            go(inner, gu_to(2, h_end, 0, 1))
            got(inner, gu_in(0, h_in))
            go(inner, gu_to(0, h_in, 2, 0))

        attend(0, rank(i))

        @pl.when(i == 3)
        def _():
            got(end, gu_in(1, my_h))
            go(None, gu_over(twin))
            got(inner, gu_in(0, h_end))
            go(inner, gu_to(0, h_end, 2, 0))
            go(inner, dn_to(u, h_in, 2, 0) + dn_to(u, h_end, 2, 0))

        back = rank(i - 1)
        kv_crossed(back)
        attend(1, back)
        return carry

    lax.fori_loop(1, 4, attend_step, 0)
    kv_crossed(rank(3))
    attend(1, rank(3))

    for h in range(heads_a):
        attn[:, h * DHA:(h + 1) * DHA] = (acc_a[h] / l_a[h]).astype(BF16)
    width_a = heads_a * DHA
    for h in range(heads_b):
        attn[:, width_a + h * DHB:width_a + (h + 1) * DHB] = (acc_b[h] / l_b[h]).astype(BF16)

    def s1_copy(k):
        yy = (1 - y, y)[k]
        return remote(
            pout.at[yy], s1_in.at[yy], s1_s.at[k], s1_r.at[k], tp=tp_at(y, 1 - c)
        )

    def s2_copy():
        return remote(q1, s2_in, s2_s.at[0], s2_r.at[0], tp=tp_at(1 - y, c))

    for who, cc in enumerate((1 - c, c)):
        for k, yy in enumerate((1 - y, y)):
            block = attn[pl.ds(pl.multiple_of(tp_at(yy, cc) * own, own), own), :]
            value = (
                jnp.dot(block[:, :width_a], woa[...], preferred_element_type=F32)
                + jnp.dot(block[:, width_a:], wob[...], preferred_element_type=F32)
            )
            if who == 0:
                pout[yy] = value.astype(BF16)
                go(None, [P(s1_copy, k)])
            else:
                own1[yy] = value

    got(None, [P(s1_copy, 0)])
    q1[...] = (own1[1 - y] + s1_in[1 - y].astype(F32)).astype(BF16)
    go(None, [s2_copy])

    got(None, gu_in(2, my_h))
    go(None, gu_over(2))
    go(None, dn_over(u))
    go(inner, dn_to(u, h_end, 0, 1))
    got(inner, gu_in(3, h_end))
    go(inner, gu_to(3, h_end, 0, 1))
    got(inner, dn_in(0, h_in) + dn_in(0, h_end))
    go(inner, dn_to(0, h_in, 2, 0) + dn_to(0, h_end, 2, 0))
    got(end, dn_in(1, my_h))
    go(None, dn_over(1 - u))

    mine = pl.ds(pl.multiple_of(tp * own, own), own)
    got(None, [P(s1_copy, 1)])
    middle = x_ref[...].astype(F32) + own1[y] + s1_in[y].astype(F32)
    got(None, [s2_copy])
    middle = middle + s2_in[...].astype(F32)
    mid[...] = middle
    normed = middle * lax.rsqrt(jnp.mean(middle * middle, axis=-1, keepdims=True) + norm_eps)
    nrm[jz, mine, :] = (normed * gmid_ref[...]).astype(BF16)

    part = own // 2

    def rows_of(tt, p=None):
        if p is None:
            return pl.ds(pl.multiple_of(tt * own, own), own)
        return pl.ds(pl.multiple_of(tt * own + p * part, part), part)

    def ag_z(p, j):
        at = nrm.at[j, rows_of(tp, p)]
        return remote(at, at, agz_s.at[p], agz_r.at[p], sp=2 * mate + x)

    def ag_y(tt):
        at = nrm.at[jz, rows_of(tt)]
        return remote(at, at, agy_s.at[0], agy_r.at[0], tp=tp_at(1 - y, c))

    def ag_f(p, tt):
        at = nrm.at[1 - jz, rows_of(tt, p)]
        return remote(at, at, agf_s.at[p], agf_r.at[p], tp=tp_at(1 - y, c))

    def ag_c(k, cc):
        j, tt = ((jz, tp_at(y, cc)), (jz, tp_at(1 - y, cc)),
                 (1 - jz, tp_at(y, cc)), (1 - jz, tp_at(1 - y, cc)))[k]
        at = nrm.at[j, rows_of(tt)]
        return remote(at, at, agc_s.at[k], agc_r.at[k], tp=tp_at(y, 1 - c))

    go(None, [P(ag_z, 0, jz), P(ag_y, tp), P(ag_z, 1, jz), P(ag_c, 0, c)])

    got(None, gu_in(3, my_h))
    go(None, gu_over(3))

    for p in range(2):
        got(None, [P(ag_z, p, 1 - jz)])
        go(None, [P(ag_f, p, tp)])
    go(None, [P(ag_c, 2, c)])
    got(None, [P(ag_y, tp_at(1 - y, c))])
    go(None, [P(ag_c, 1, c)])

    def gate_up(j, col, zi):
        side = (1 - col) * x + col * (1 - x)
        columns = pl.ds(pl.multiple_of((2 * zi + side) * chunk, chunk), chunk)
        weights = gux[zi] if col else gub[zi, my_h]
        acc[j] += jnp.dot(nrm[j, :, columns], weights, preferred_element_type=F32)

    def gu_crossed(zi):
        for p in everyp:
            cut = pl.ds(p * gr, gr)
            remote(
                gub.at[zi, my_h, cut], gux.at[zi, cut],
                gux_s.at[zi, p], gux_r.at[zi, p], sp=2 * z + 1 - x,
            ).wait_recv()

    acc[...] = jnp.zeros_like(acc)
    got(None, [P(ag_c, 0, 1 - c), P(ag_c, 1, 1 - c)])

    def near_rows(k, carry):
        zi = rank(k)
        gate_up(jz, 0, zi)
        gu_crossed(zi)
        gate_up(jz, 1, zi)
        return carry

    def other_rows(k, carry):
        zi = rank(k)
        gate_up(1 - jz, 0, zi)
        gate_up(1 - jz, 1, zi)
        return carry

    lax.fori_loop(0, 2, near_rows, 0)
    for p in range(2):
        got(None, [P(ag_f, p, tp_at(1 - y, c))])
    go(None, [P(ag_c, 3, c)])
    lax.fori_loop(2, 3, near_rows, 0)
    got(None, [P(ag_c, 2, 1 - c), P(ag_c, 3, 1 - c)])
    lax.fori_loop(0, 3, other_rows, 0)
    last = mz(3)
    gate_up(jz, 0, last)
    gate_up(1 - jz, 0, last)
    gu_crossed(last)
    gate_up(jz, 1, last)
    gate_up(1 - jz, 1, last)

    def edge_x():
        return remote(eg_out, eg_x, eg_s.at[0], eg_r.at[0], sp=2 * z + 1 - x)

    def edge_p():
        return remote(eg_out, eg_p, eg_s.at[1], eg_r.at[1], sp=2 * far + 1 - x)

    rim = [acc[j, at:at + 1, :] for j in range(2) for at in (0, rows - 1)]
    rim.append(jnp.zeros((eg_out.shape[0] - 4, 2 * ff), F32))
    eg_out[...] = jnp.concatenate(rim, axis=0).astype(BF16)
    go(None, [edge_x])
    go(cross == 1, [edge_p])

    @pl.when(cross == 0)
    def _():
        eg_p[...] = jnp.zeros_like(eg_p)

    got(inner, dn_in(2, h_end))
    go(inner, dn_to(2, h_end, 0, 1))
    got(None, dn_in(2, my_h))
    go(None, dn_over(2))

    got(None, [edge_x])
    got(cross == 1, [edge_p])

    is_right = x == 1

    def convolved(j, lane, taps_ref):
        cut = slice(lane, lane + ff)
        now = acc[j, :, cut].astype(BF16).astype(F32)
        beside = eg_x[:, cut].astype(F32)
        beyond = eg_p[:, cut].astype(F32)
        if j == 0:
            low = jnp.where(is_right, beside[1:2], beyond[3:4])
            high = jnp.where(is_right, beside[2:3], beside[0:1])
        else:
            low = jnp.where(is_right, beside[3:4], beside[1:2])
            high = jnp.where(is_right, beyond[0:1], beside[2:3])
        line = lax.broadcasted_iota(jnp.int32, now.shape, 0)
        before = jnp.where(line == 0, low, pltpu.roll(now, 1, 0))
        after = jnp.where(line == rows - 1, high, pltpu.roll(now, rows - 1, 0))
        taps = taps_ref[:, pl.ds(pl.multiple_of(my_h * ff, ff), ff)]
        return before * taps[0:1] + now * taps[1:2] + after * taps[2:3]

    for j in range(2):
        gate = convolved(j, 0, cg_ref)
        out = (gate / (1.0 + jnp.exp(-gate)) * convolved(j, ff, cu_ref)).astype(BF16)
        for yy in range(2):
            for cc in range(2):
                at = tp_at(yy, cc) * own
                to = (j * 2 + yy) * own
                hid[cc, to:to + own, :] = out[at:at + own]

    def d1_copy(b):
        return remote(p2.at[b], s2a.at[b], d1_s.at[b], d1_r.at[b], tp=tp_at(y, 1 - c))

    def d2_copy(b, k):
        jj, yy = ((jz, 1 - y), (1 - jz, y), (1 - jz, 1 - y))[k]
        where = ({"tp": tp_at(1 - y, c)}, {"sp": 2 * mate + x},
                 {"sp": 2 * mate + x, "tp": tp_at(1 - y, c)})[k]
        return remote(
            q2.at[b, 2 * jj + yy], s2b.at[b, k], d2_s.at[b, k], d2_r.at[b, k], **where
        )

    def block_of(col, vb):
        side = (1 - col) * x + col * (1 - x)
        return 2 * mz(vb) + side

    def first_sum(col, vb):
        b = block_of(col, vb)
        weights = dnx[mz(vb)] if col else dnb[mz(vb), my_h]
        p2[b] = jnp.dot(hid[1 - c], weights, preferred_element_type=F32).astype(BF16)
        go(None, [P(d1_copy, b)])
        own2[b] = jnp.dot(hid[c], weights, preferred_element_type=F32)

    def second_sum(col, vb):
        b = block_of(col, vb)
        got(None, [P(d1_copy, b)])
        value = own2[b] + s2a[b].astype(F32)
        own2[b] = value
        short = value.astype(BF16)
        for k in range(4):
            q2[b, k] = short[k * own:(k + 1) * own]
        go(None, [P(d2_copy, b, k) for k in (2, 0, 1)])

    def down(k):
        first_sum(0, ranks[k])
        got(None, dn_over(ranks[k]))
        first_sum(1, ranks[k])

    def pass_on(k):
        second_sum(0, ranks[k])
        second_sum(1, ranks[k])

    down(0)
    down(1)
    pass_on(0)
    down(2)
    pass_on(1)
    pass_on(2)
    got(inner, dn_in(3, h_end))
    go(inner, dn_to(3, h_end, 0, 1))
    got(None, dn_in(3, my_h))
    go(None, dn_over(3))
    down(3)
    pass_on(3)

    dcols = dnx.shape[2]
    here = pl.ds(pl.multiple_of((2 * jz + y) * own, own), own)

    for b in range(own2.shape[0]):
        got(None, [P(d2_copy, b, i) for i in range(3)])
        cut = slice(b * dcols, (b + 1) * dcols)
        value = own2[b, here, :]
        for i in range(3):
            value = value + s2b[b, i].astype(F32)
        out_ref[:, cut] = (mid[:, cut] + value).astype(out_ref.dtype)

    for cond, copies in sent:
        def run(copies=copies):
            for copy in copies:
                copy().wait_send()
        under(cond, run)


def on_device(n, tp_n, *args):
    (x_res, q_a, k_a, v_a, q_b, k_b, v_b, gain_qa, gain_ka, gain_qb, gain_kb, w_out_a, w_out_b,
     gain_mid, w_gate, w_up, conv_gate, conv_up, w_down) = args
    ff = w_gate.shape[1] // 2
    chunk, dcols = w_gate.shape[0], w_down.shape[1]
    if n != 8 or tp_n != 4 or chunk % 128 or dcols % 128 or w_gate.shape[1] % 256:
        return on_device_narrow(*args)
    rows = q_a.shape[0]
    own, width = x_res.shape
    heads_a, heads_b = q_a.shape[1] // DHA, q_b.shape[1] // DHB
    freq_a, freq_b = lane_frequencies(DHA, 2 * DHA), lane_frequencies(DHB, DHB)
    vmem = pl.BlockSpec(memory_space=pltpu.VMEM)
    hbm = pl.BlockSpec(memory_space=pltpu.MemorySpace.HBM)
    kv_width = 2 * k_a.shape[1] + 2 * k_b.shape[1]
    dma = pltpu.SemaphoreType.DMA
    scratch = [
        pltpu.VMEM((2, 4, rows, kv_width), BF16),
        pltpu.VMEM((heads_a, rows, DHA), BF16),
        pltpu.VMEM((heads_b, rows, DHB), BF16),
        pltpu.VMEM((heads_a, rows, 1), F32),
        pltpu.VMEM((heads_a, rows, 1), F32),
        pltpu.VMEM((heads_a, rows, DHA), F32),
        pltpu.VMEM((heads_b, rows, 1), F32),
        pltpu.VMEM((heads_b, rows, 1), F32),
        pltpu.VMEM((heads_b, rows, DHB), F32),
        pltpu.VMEM(w_out_a.shape, BF16),
        pltpu.VMEM(w_out_b.shape, BF16),
        pltpu.VMEM((4, 2, chunk, 2 * ff), BF16),
        pltpu.VMEM((4, chunk, 2 * ff), BF16),
        pltpu.VMEM((4, 2, ff, dcols), BF16),
        pltpu.VMEM((4, ff, dcols), BF16),
        pltpu.VMEM((rows, q_a.shape[1] + q_b.shape[1]), BF16),
        pltpu.VMEM((2, own, width), BF16),
        pltpu.VMEM((2, own, width), F32),
        pltpu.VMEM((2, own, width), BF16),
        pltpu.VMEM((own, width), BF16),
        pltpu.VMEM((own, width), BF16),
        pltpu.VMEM((own, width), F32),
        pltpu.VMEM((2, rows, width), BF16),
        pltpu.VMEM((2, rows, 2 * ff), F32),
        pltpu.VMEM((16, 2 * ff), BF16),
        pltpu.VMEM((16, 2 * ff), BF16),
        pltpu.VMEM((16, 2 * ff), BF16),
        pltpu.VMEM((2, rows, ff), BF16),
        pltpu.VMEM((n, rows, dcols), BF16),
        pltpu.VMEM((n, rows, dcols), F32),
        pltpu.VMEM((n, rows, dcols), BF16),
        pltpu.VMEM((n, 4, own, dcols), BF16),
        pltpu.VMEM((n, 3, own, dcols), BF16),
        dma((8,)),
        dma((2, 4)), dma((4,)), dma((4,)), dma((4,)),
        dma((2, 4, 2, GU_PIECES)), dma((4, 2, GU_PIECES)), dma((4, GU_PIECES)), dma((4, GU_PIECES)),
        dma((2, 4, 2, DN_PIECES)), dma((4, 2, DN_PIECES)), dma((4, DN_PIECES)), dma((4, DN_PIECES)),
        dma((2,)), dma((2,)), dma((1,)), dma((1,)),
        dma((2,)), dma((2,)), dma((1,)), dma((1,)), dma((2,)), dma((2,)), dma((4,)), dma((4,)),
        dma((2,)), dma((2,)),
        dma((n,)), dma((n,)), dma((n, 3)), dma((n, 3)),
    ]
    return pl.pallas_call(
        kernel,
        out_shape=jax.ShapeDtypeStruct(x_res.shape, BF16),
        in_specs=[vmem] * 13 + [hbm, hbm, vmem, hbm, hbm, vmem, vmem, hbm],
        out_specs=vmem,
        scratch_shapes=scratch,
        compiler_params=pltpu.CompilerParams(
            collective_id=0, has_side_effects=True, vmem_limit_bytes=60 * 1024 * 1024
        ),
        name="layer",
    )(
        x_res, q_a, jnp.transpose(k_a), jnp.transpose(v_a), q_b, k_b, v_b,
        gain_qa[None], gain_ka[None], gain_qb[None], gain_kb[None],
        freq_a, freq_b,
        w_out_a, w_out_b, gain_mid[None], w_gate, w_up, conv_gate, conv_up, w_down,
    )


def extended(block, sides, width):
    for axis, dim in sides:
        count = lax.axis_size(axis)
        forward = [(i, i + 1) for i in range(count - 1)]
        backward = [(target, source) for source, target in forward]
        low = lax.ppermute(
            lax.slice_in_dim(block, block.shape[dim] - width, None, axis=dim), axis, forward
        )
        high = lax.ppermute(lax.slice_in_dim(block, 0, width, axis=dim), axis, backward)
        block = jnp.concatenate([low, block, high], axis=dim)
    return block


def rotate_half(values):
    first, second = jnp.split(values, 2, axis=-1)
    return jnp.concatenate([-second, first], axis=-1)


def prepare(raw, gain, head_size, positions):
    count = raw.shape[0]
    heads = raw.shape[1] // head_size
    values = raw.astype(jnp.float32).reshape(count, heads, head_size)
    values = values * lax.rsqrt(jnp.mean(values * values, axis=-1, keepdims=True) + norm_eps)
    values = values * gain
    angles = rotary_angles(positions, head_size)
    cosine, sine = jnp.cos(angles), jnp.sin(angles)
    row_part, col_part = jnp.split(values, 2, axis=-1)
    turned = jnp.concatenate([rotate_half(row_part), rotate_half(col_part)], axis=-1)
    values = values * cosine[:, None, :] + turned * sine[:, None, :]
    return values.astype(jnp.bfloat16)


def start_state(queries):
    count, kv_heads, groups, head_size = queries.shape
    lowest = jnp.full((kv_heads, groups, count), -1e30, jnp.float32)
    totals = jnp.zeros((kv_heads, groups, count), jnp.float32)
    summed = jnp.zeros((kv_heads, groups, count, head_size), jnp.float32)
    return (lowest, totals, summed)


def attend(state, queries, key_piece, value_piece):
    head_size = queries.shape[3]
    kv_heads = queries.shape[1]
    length = key_piece.shape[0]
    keys = key_piece.reshape(length, kv_heads, head_size)
    values = value_piece.reshape(length, kv_heads, head_size)
    span = length
    while span > 1024 and span % 2 == 0:
        span = span // 2
    scale = jnp.float32(head_size ** (-0.5))

    def one_span(index, carry):
        running, totals, summed = carry
        key_rows = lax.dynamic_slice_in_dim(keys, index * span, span, 0)
        value_rows = lax.dynamic_slice_in_dim(values, index * span, span, 0)
        scores = (
            jnp.einsum("qkgd,skd->kgqs", queries, key_rows, preferred_element_type=jnp.float32)
            * scale
        )
        highest = jnp.maximum(running, jnp.max(scores, axis=-1))
        factor = jnp.exp(running - highest)
        expd = jnp.exp(scores - highest[..., None])
        totals = totals * factor + jnp.sum(expd, axis=-1)
        summed = summed * factor[..., None] + jnp.einsum(
            "kgqs,skd->kgqd",
            expd.astype(jnp.bfloat16),
            value_rows,
            preferred_element_type=jnp.float32,
        )
        return (highest, totals, summed)

    return lax.fori_loop(0, length // span, one_span, state)


def finish(state):
    running, totals, summed = state
    kv_heads, groups, count, head_size = summed.shape
    result = summed / totals[..., None]
    return (
        jnp.transpose(result, (2, 0, 1, 3))
        .reshape(count, kv_heads * groups * head_size)
        .astype(jnp.bfloat16)
    )


def on_device_narrow(
    x_res,
    q_a,
    k_a,
    v_a,
    q_b,
    k_b,
    v_b,
    gain_qa,
    gain_ka,
    gain_qb,
    gain_kb,
    w_out_a,
    w_out_b,
    gain_mid,
    w_gate,
    w_up,
    conv_gate,
    conv_up,
    w_down,
):
    tok_rows = q_a.shape[0]
    whole_gate, whole_up, whole_down = (
        lax.all_gather(w_gate, "sp", axis=0, tiled=True),
        lax.all_gather(w_up, "sp", axis=0, tiled=True),
        lax.all_gather(w_down, "sp", axis=1, tiled=True),
    )
    positions = lax.axis_index("sp") * tok_rows + lax.iota(jnp.int32, tok_rows)
    kv_a = k_a.shape[1] // DHA
    kv_b = k_b.shape[1] // DHB
    query_a = prepare(q_a, gain_qa, DHA, positions)
    query_a = query_a.reshape(tok_rows, kv_a, query_a.shape[1] // kv_a, DHA)
    query_b = prepare(q_b, gain_qb, DHB, positions)
    query_b = query_b.reshape(tok_rows, kv_b, query_b.shape[1] // kv_b, DHB)
    keys_a = prepare(k_a, gain_ka, DHA, positions).reshape(tok_rows, kv_a * DHA)
    keys_b = prepare(k_b, gain_kb, DHB, positions).reshape(tok_rows, kv_b * DHB)
    state_a = attend(
        start_state(query_a),
        query_a,
        lax.all_gather(keys_a, "sp", axis=0, tiled=True),
        lax.all_gather(v_a, "sp", axis=0, tiled=True),
    )
    state_b = attend(
        start_state(query_b),
        query_b,
        lax.all_gather(keys_b, "sp", axis=0, tiled=True),
        lax.all_gather(v_b, "sp", axis=0, tiled=True),
    )
    attn_a = finish(state_a)
    attn_b = finish(state_b)
    projected = lax.psum_scatter(
        (
            jnp.dot(attn_a, w_out_a, preferred_element_type=jnp.float32)
            + jnp.dot(attn_b, w_out_b, preferred_element_type=jnp.float32)
        ).astype(jnp.bfloat16),
        "tp",
        scatter_dimension=0,
        tiled=True,
    ).astype(jnp.float32)
    middle = x_res.astype(jnp.float32) + projected
    normed = middle * lax.rsqrt(jnp.mean(middle * middle, axis=-1, keepdims=True) + norm_eps)
    normed = (normed * gain_mid).astype(jnp.bfloat16)
    gathered = lax.all_gather(normed, "tp", axis=0, tiled=True)
    gate_pre = jnp.dot(gathered, whole_gate, preferred_element_type=jnp.float32)
    up_pre = jnp.dot(gathered, whole_up, preferred_element_type=jnp.float32)
    width = gate_pre.shape[1]
    joined = jnp.concatenate([gate_pre, up_pre], axis=1).astype(jnp.bfloat16)
    padded = extended(joined, (("sp", 0),), 1)
    taps = jnp.concatenate([conv_gate, conv_up], axis=1)
    mixed = padded[:-2] * taps[0] + padded[1:-1] * taps[1] + padded[2:] * taps[2]
    hidden = (jax.nn.silu(mixed[:, :width]) * mixed[:, width:]).astype(jnp.bfloat16)
    terms = jnp.dot(hidden, whole_down, preferred_element_type=jnp.float32)
    summed = lax.psum_scatter(
        terms.astype(jnp.bfloat16), "tp", scatter_dimension=0, tiled=True
    ).astype(jnp.float32)
    return (middle + summed).astype(jnp.bfloat16)


def solution(mesh):
    in_specs = (
        P(("sp", "tp"), None),
        P("sp", "tp"),
        P("sp", "tp"),
        P("sp", "tp"),
        P("sp", "tp"),
        P("sp", "tp"),
        P("sp", "tp"),
        P(),
        P(),
        P(),
        P(),
        P("tp", None),
        P("tp", None),
        P(),
        P("sp", "tp"),
        P("sp", "tp"),
        P(None, "tp"),
        P(None, "tp"),
        P("tp", "sp"),
    )
    out_specs = P(("sp", "tp"), None)
    body = functools.partial(on_device, mesh.shape["sp"], mesh.shape["tp"])
    return jax.shard_map(
        body, mesh=mesh, in_specs=in_specs, out_specs=out_specs, check_vma=False
    )
```

```python
import functools

import jax
import jax.numpy as jnp
import numpy as np
from jax import lax
from jax.experimental import pallas as pl
from jax.experimental.pallas import tpu as pltpu
from jax.sharding import PartitionSpec as P

DHA = 64
DHB = 128

norm_eps = 1e-06
rope_theta = 10000.0
F32 = jnp.float32
BF16 = jnp.bfloat16
MESH = pl.DeviceIdType.MESH
GU_PIECES = 4
DN_PIECES = 2
LOG2E = 1.4426950408889634
PAIRED = True
TAIL = 1


def rotary_angles(positions, head_size):
    half = head_size // 2
    inverse = jnp.power(jnp.float32(rope_theta), -jnp.arange(0, half, 2, dtype=jnp.float32) / half)
    grid_row = (positions // 64).astype(jnp.float32)[:, None] * inverse[None, :]
    grid_col = (positions % 64).astype(jnp.float32)[:, None] * inverse[None, :]
    return jnp.concatenate([grid_row, grid_row, grid_col, grid_col], axis=-1)


def lane_frequencies(head_size, width):
    half = head_size // 2
    steps = -np.arange(0, half, 2, dtype=np.float32) / np.float32(half)
    inverse = np.power(np.float32(rope_theta), steps).astype(np.float32)
    return jnp.asarray(np.tile(inverse, width // inverse.shape[0])[None])


def block_mean(width, head):
    i = lax.broadcasted_iota(jnp.int32, (width, width), 0)
    j = lax.broadcasted_iota(jnp.int32, (width, width), 1)
    return jnp.where(lax.div(i, head) == lax.div(j, head), F32(1.0 / head), F32(0.0))


def block_turn(width, head):
    quarter = head // 4
    i = lax.broadcasted_iota(jnp.int32, (width, width), 0)
    j = lax.broadcasted_iota(jnp.int32, (width, width), 1)
    first = lax.rem(j, 2 * quarter) < quarter
    return jnp.where(
        first & (i == j + quarter),
        F32(-1.0),
        jnp.where(jnp.logical_not(first) & (i == j - quarter), F32(1.0), F32(0.0)),
    )


def exact_dot(a, b):
    return jnp.dot(a, b, precision=lax.Precision.HIGHEST, preferred_element_type=F32)


def prepared(raw, gain, angle_cos, angle_sin, head):
    width = raw.shape[1]
    values = raw.astype(F32)
    values = values * lax.rsqrt(exact_dot(values * values, block_mean(width, head)) + norm_eps)
    values = values * gain
    turned = exact_dot(values, block_turn(width, head))
    return (values * angle_cos + turned * angle_sin).astype(BF16)


def kernel(
    x_ref, qa_ref, kat_ref, vat_ref, qb_ref, kb_ref, vb_ref,
    gqa_ref, gka_ref, gqb_ref, gkb_ref,
    fra_ref, frb_ref,
    woa_hbm, wob_hbm, gmid_ref, wg_hbm, wu_hbm, cg_ref, cu_ref, wd_hbm,
    out_ref,
    kv, qas, qbs, m_a, acc_a, m_b, acc_b,
    woa, wob, gub, gux, dnb, dnx,
    attn, pout, own1, s1_in, q1, s2_in, mid, nrm, acc, eg_out, eg_x, eg_p, hid,
    p2, own2, s2a, q2, s2b,
    loc_sem, kvz_s, kvz_r, kvx_s, kvx_r, guz_s, guz_r, gux_s, gux_r,
    dnz_s, dnz_r, dnx_s, dnx_r, s1_s, s1_r, s2_s, s2_r,
    agz_s, agz_r, agy_s, agy_r, agf_s, agf_r, agc_s, agc_r, eg_s, eg_r,
    d1_s, d1_r, d2_s, d2_r,
):
    sp = lax.axis_index("sp")
    tp = lax.axis_index("tp")
    z, x = lax.div(sp, 2), lax.rem(sp, 2)
    y, c = lax.div(tp, 2), lax.rem(tp, 2)
    rows = qa_ref.shape[0]
    own = x_ref.shape[0]
    chunk, ff = gub.shape[2], gub.shape[3] // 2
    flip = lax.div(z, 2)

    def mz(v):
        return (1 - flip) * v + flip * (3 - v)

    u = mz(z)
    inner, end = u == 1, u == 0
    mate = mz(1 - u)
    my_h = lax.rem(z, 2)
    jz = my_h
    h_end, h_in = lax.rem(mz(0), 2), lax.rem(mz(1), 2)
    cross = lax.rem(x + flip, 2)
    far = 2 * (1 - flip) * 2 - 2 + z
    twin = 1 - u
    ranks = [u, twin, 2, 3]

    def tp_at(yy, cc):
        return yy * 2 + cc

    barrier = pltpu.get_barrier_semaphore()
    greet = [
        (None, {"sp": 2 * z + 1 - x}),
        (None, {"tp": tp_at(y, 1 - c)}),
        (None, {"tp": tp_at(1 - y, c)}),
        (None, {"sp": 2 * mate + x}),
        (None, {"sp": 2 * mate + x, "tp": tp_at(1 - y, c)}),
        (inner, {"sp": 2 * mz(2) + x}),
        (cross == 1, {"sp": 2 * far + 1 - x}),
    ]
    for cond, where in greet:
        def signal(where=where):
            pl.semaphore_signal(barrier, inc=1, device_id=where, device_id_type=MESH)
        if cond is None:
            signal()
        else:
            pl.when(cond)(signal)

    loc = []
    for h in range(2):
        cut = pl.ds(h * ff, ff)
        loc.append(pltpu.make_async_copy(
            wg_hbm.at[:, cut], gub.at[z, h, :, pl.ds(0, ff)], loc_sem.at[len(loc)]))
        loc.append(pltpu.make_async_copy(
            wu_hbm.at[:, cut], gub.at[z, h, :, pl.ds(ff, ff)], loc_sem.at[len(loc)]))
    for h in range(2):
        loc.append(pltpu.make_async_copy(
            wd_hbm.at[pl.ds(h * ff, ff)], dnb.at[z, h], loc_sem.at[len(loc)]))
    loc.append(pltpu.make_async_copy(woa_hbm, woa, loc_sem.at[len(loc)]))
    loc.append(pltpu.make_async_copy(wob_hbm, wob, loc_sem.at[len(loc)]))
    for copy in loc:
        copy.start()

    def remote(src, dst, send, recv, **where):
        return pltpu.make_async_remote_copy(
            src_ref=src, dst_ref=dst, send_sem=send, recv_sem=recv,
            device_id=where, device_id_type=MESH,
        )

    sent = []

    def under(cond, run):
        if cond is None:
            run()
        else:
            pl.when(cond)(run)

    def go(cond, copies):
        def run():
            for copy in copies:
                copy().start()
        under(cond, run)
        sent.append((cond, copies))

    def got(cond, copies):
        def run():
            for copy in copies:
                copy().wait_recv()
        under(cond, run)

    def relay(cond, arriving, *leaving):
        def run():
            for k, copy in enumerate(arriving):
                copy().wait_recv()
                for copies in leaving:
                    copies[k]().start()
        under(cond, run)
        for copies in leaving:
            sent.append((cond, copies))

    P = functools.partial
    gr, dr = chunk // GU_PIECES, ff // DN_PIECES
    everyp, everyd = range(GU_PIECES), range(DN_PIECES)

    def kv_z(vb, to, way):
        zi = mz(vb)
        return remote(kv.at[0, zi], kv.at[0, zi], kvz_s.at[way, zi], kvz_r.at[zi], sp=2 * mz(to) + x)

    def kv_x(vb):
        zi = mz(vb)
        return remote(kv.at[0, zi], kv.at[1, zi], kvx_s.at[zi], kvx_r.at[zi], sp=2 * z + 1 - x)

    def gu_z(vb, h, p, to, way):
        zi, cut = mz(vb), pl.ds(p * gr, gr)
        return remote(
            gub.at[zi, h, cut], gub.at[zi, h, cut],
            guz_s.at[way, zi, h, p], guz_r.at[zi, h, p], sp=2 * mz(to) + x,
        )

    def gu_x(vb, p):
        zi, cut = mz(vb), pl.ds(p * gr, gr)
        return remote(
            gub.at[zi, my_h, cut], gux.at[zi, cut],
            gux_s.at[zi, p], gux_r.at[zi, p], sp=2 * z + 1 - x,
        )

    def dn_z(vb, h, p, to, way):
        zi, cut = mz(vb), pl.ds(p * dr, dr)
        return remote(
            dnb.at[zi, h, cut], dnb.at[zi, h, cut],
            dnz_s.at[way, zi, h, p], dnz_r.at[zi, h, p], sp=2 * mz(to) + x,
        )

    def dn_x(vb, p):
        zi, cut = mz(vb), pl.ds(p * dr, dr)
        return remote(
            dnb.at[zi, my_h, cut], dnx.at[zi, cut],
            dnx_s.at[zi, p], dnx_r.at[zi, p], sp=2 * z + 1 - x,
        )

    def gu_to(vb, h, to, way, pieces=everyp):
        return [P(gu_z, vb, h, p, to, way) for p in pieces]

    def dn_to(vb, h, to, way):
        return [P(dn_z, vb, h, p, to, way) for p in everyd]

    def gu_over(vb, pieces=everyp):
        return [P(gu_x, vb, p) for p in pieces]

    def dn_over(vb):
        return [P(dn_x, vb, p) for p in everyd]

    def gu_in(vb, h):
        return [P(gu_z, vb, h, p, 1 - u, 0) for p in everyp]

    def dn_in(vb, h):
        return [P(dn_z, vb, h, p, 1 - u, 0) for p in everyd]

    def kv_in(vb):
        return [P(kv_z, vb, 1 - u, 0)]

    for copy in loc[:4]:
        copy.wait()
    pl.semaphore_wait(barrier, 5 + u + cross)
    go(inner, gu_to(u, h_in, 2, 0, [0, 1]))
    go(inner, gu_to(u, h_end, 0, 1, [0, 1]))
    go(end, gu_to(u, h_in, 1, 0, [0]))
    go(None, gu_over(u, [0, 1]))

    def tables(freq_ref, head):
        shape = (rows, freq_ref.shape[1])
        token = lax.broadcasted_iota(jnp.int32, shape, 0) + sp * rows
        lane = lax.broadcasted_iota(jnp.int32, shape, 1)
        grid = jnp.where(lax.rem(lane, head) < head // 2, lax.div(token, 64), lax.rem(token, 64))
        angles = grid.astype(F32) * freq_ref[...]
        return jnp.cos(angles), jnp.sin(angles)

    ca, sa = tables(fra_ref, DHA)
    cb, sb = tables(frb_ref, DHB)
    wka, wkb = kat_ref.shape[0], kb_ref.shape[1]

    def wide(table, width):
        if width <= table.shape[1]:
            return table[:, :width]
        return jnp.concatenate([table] * (width // table.shape[1]), axis=1)

    def gains(ref, width):
        g = ref[...]
        count = width // g.shape[1]
        return g if count == 1 else jnp.concatenate([g] * count, axis=1)

    raw_a = jnp.transpose(kat_ref[...].astype(F32))
    val_a = jnp.transpose(vat_ref[...].astype(F32)).astype(BF16)
    keys_a = prepared(raw_a, gains(gka_ref, wka), wide(ca, wka), wide(sa, wka), DHA)
    keys_b = prepared(kb_ref[...], gains(gkb_ref, wkb), wide(cb, wkb), wide(sb, wkb), DHB)
    kv[0, z, :, :wkb] = keys_b
    kv[0, z, :, wkb:2 * wkb] = vb_ref[...]
    kv[0, z, :, 2 * wkb:] = jnp.concatenate([keys_a, val_a], axis=1)

    go(inner, [P(kv_z, u, 2, 0), P(kv_z, u, 0, 1)])
    go(end, [P(kv_z, u, 1, 0)])
    go(None, [P(kv_x, u)])
    go(end, gu_to(u, h_in, 1, 0, everyp[1:]) + gu_to(u, h_end, 1, 0))
    for copy in loc[4:]:
        copy.wait()
    go(end, dn_to(u, h_in, 1, 0) + dn_to(u, h_end, 1, 0))

    heads_a = qa_ref.shape[1] // DHA
    heads_b = qb_ref.shape[1] // DHB
    qa = prepared(
        qa_ref[...], gains(gqa_ref, heads_a * DHA), wide(ca, heads_a * DHA),
        wide(sa, heads_a * DHA), DHA,
    )
    qb = prepared(
        qb_ref[...], gains(gqb_ref, heads_b * DHB), wide(cb, heads_b * DHB),
        wide(sb, heads_b * DHB), DHB,
    )
    for h in range(heads_a):
        qas[h] = jnp.concatenate([qa[:, h * DHA:(h + 1) * DHA], jnp.zeros((rows, wka), BF16)], axis=1)
    for h in range(heads_b):
        qbs[h] = qb[:, h * DHB:(h + 1) * DHB]
    for ref, low in ((m_a, -1e30), (m_b, -1e30), (acc_a, 0.0), (acc_b, 0.0)):
        ref[...] = jnp.full(ref.shape, low, F32)

    def attend_one(query, keys, values, head, m, total, h):
        scale = F32(head ** (-0.5) * LOG2E)
        scores = [
            lax.dot_general(
                query, key, (((1,), (1,)), ((), ())), preferred_element_type=F32
            ) * scale
            for key in keys
        ]
        most = functools.reduce(jnp.maximum, scores)
        before = m[h]
        highest = jnp.maximum(before, jnp.max(most, axis=-1, keepdims=True))
        factor = jnp.exp2(before - highest)
        level = wide_to(highest, most.shape[1])
        added = functools.reduce(jnp.add, [
            jnp.dot(jnp.exp2(score - level).astype(BF16), value, preferred_element_type=F32)
            for score, value in zip(scores, values)
        ])
        total[h] = total[h] * wide_to(factor, added.shape[1]) + added
        m[h] = highest

    def wide_to(table, width):
        return jnp.concatenate([table] * (width // table.shape[1]), axis=1)

    ones_b = jnp.ones((rows, wkb), BF16)
    is_key = lax.broadcasted_iota(jnp.int32, (rows, 2 * wka), 1) < wka

    def attend(*blocks):
        keys = [kv[col, zi, :, :wkb] for col, zi in blocks]
        values = [
            jnp.concatenate([kv[col, zi, :, wkb:2 * wkb], ones_b], axis=1) for col, zi in blocks
        ]
        for h in range(heads_b):
            attend_one(qbs[h], keys, values, DHB, m_b, acc_b, h)
        keys = [kv[col, zi, :, 2 * wkb:] for col, zi in blocks]
        values = [jnp.where(is_key, BF16(1.0), pair) for pair in keys]
        for h in range(heads_a):
            attend_one(qas[h], keys, values, DHA, m_a, acc_a, h)

    def rank(k):
        high = k // 2 if isinstance(k, int) else lax.div(k, 2)
        return mz(high * k + (1 - high) * (k + u - 2 * k * u))

    attend((0, z))

    def kv_crossed(zi):
        remote(
            kv.at[0, zi], kv.at[1, zi], kvx_s.at[zi], kvx_r.at[zi], sp=2 * z + 1 - x
        ).wait_recv()

    def attend_step(i, carry):
        @pl.when(i == 1)
        def _():
            got(None, kv_in(twin))
            go(inner, [P(kv_z, 0, 2, 0)])
            go(None, [P(kv_x, twin)])
            got(inner, kv_in(2))
            go(inner, [P(kv_z, 2, 0, 1), P(kv_x, 2)])
            go(inner, gu_to(u, h_in, 2, 0, everyp[2:]) + gu_to(u, h_end, 0, 1, [2]))
            go(end, gu_over(u, [2]))

        @pl.when(i == 2)
        def _():
            got(end, kv_in(2))
            go(end, [P(kv_x, 2)])
            got(inner, kv_in(3))
            go(inner, [P(kv_z, 3, 0, 1), P(kv_x, 3)])
            go(inner, gu_to(u, h_end, 0, 1, everyp[3:]) + gu_over(u, [2]))
            go(None, gu_over(u, everyp[3:]))
            relay(inner, gu_in(0, h_in), gu_to(0, h_in, 2, 0), gu_over(twin))
            go(inner, gu_to(u, h_end, 2, 0))

        @pl.when(i == 3)
        def _():
            got(end, kv_in(3))
            go(end, [P(kv_x, 3)])
            relay(inner, gu_in(2, h_end), gu_to(2, h_end, 0, 1))

        if not PAIRED:
            attend((0, rank(i)))

        @pl.when(i == 3)
        def _():
            relay(end, gu_in(1, my_h), gu_over(twin))
            relay(inner, gu_in(0, h_end), gu_to(0, h_end, 2, 0))
            go(inner, dn_to(u, h_in, 2, 0))

        back = rank(i - 1)
        kv_crossed(back)
        if PAIRED:
            attend((0, rank(i)), (1, back))
        else:
            attend((1, back))
        return carry

    lax.fori_loop(1, 4, attend_step, 0)
    kv_crossed(rank(3))
    attend((1, rank(3)))

    relay(inner, gu_in(3, h_end), gu_to(3, h_end, 0, 1))
    got(inner, dn_in(0, h_in))
    go(inner, dn_to(0, h_in, 2, 0) + dn_to(u, h_end, 2, 0))
    go(None, dn_over(u))

    for h in range(heads_a):
        both = acc_a[h]
        attn[:, h * DHA:(h + 1) * DHA] = (both[:, wka:] / both[:, :wka]).astype(BF16)
    width_a = heads_a * DHA
    for h in range(heads_b):
        attn[:, width_a + h * DHB:width_a + (h + 1) * DHB] = (
            acc_b[h, :, :wkb] / acc_b[h, :, wkb:]
        ).astype(BF16)

    def s1_copy(k):
        yy = (1 - y, y)[k]
        return remote(
            pout.at[yy], s1_in.at[yy], s1_s.at[k], s1_r.at[k], tp=tp_at(y, 1 - c)
        )

    def s2_copy():
        return remote(q1, s2_in, s2_s.at[0], s2_r.at[0], tp=tp_at(1 - y, c))

    for who, cc in enumerate((1 - c, c)):
        for k, yy in enumerate((1 - y, y)):
            block = attn[pl.ds(pl.multiple_of(tp_at(yy, cc) * own, own), own), :]
            value = (
                jnp.dot(block[:, :width_a], woa[...], preferred_element_type=F32)
                + jnp.dot(block[:, width_a:], wob[...], preferred_element_type=F32)
            )
            if who == 0:
                pout[yy] = value.astype(BF16)
                go(None, [P(s1_copy, k)])
            else:
                own1[yy] = value

    got(None, [P(s1_copy, 0)])
    q1[...] = (own1[1 - y] + s1_in[1 - y].astype(F32)).astype(BF16)
    go(None, [s2_copy])

    relay(None, gu_in(2, my_h), gu_over(2))
    got(inner, dn_in(0, h_end))
    go(inner, dn_to(0, h_end, 2, 0) + dn_to(u, h_end, 0, 1) + dn_over(twin))

    mine = pl.ds(pl.multiple_of(tp * own, own), own)
    got(None, [P(s1_copy, 1)])
    middle = x_ref[...].astype(F32) + own1[y] + s1_in[y].astype(F32)
    got(None, [s2_copy])
    middle = middle + s2_in[...].astype(F32)
    mid[...] = middle
    normed = middle * lax.rsqrt(jnp.mean(middle * middle, axis=-1, keepdims=True) + norm_eps)
    nrm[jz, mine, :] = (normed * gmid_ref[...]).astype(BF16)

    part = own // 2

    def rows_of(tt, p=None):
        if p is None:
            return pl.ds(pl.multiple_of(tt * own, own), own)
        return pl.ds(pl.multiple_of(tt * own + p * part, part), part)

    def ag_z(p, j):
        at = nrm.at[j, rows_of(tp, p)]
        return remote(at, at, agz_s.at[p], agz_r.at[p], sp=2 * mate + x)

    def ag_y(tt):
        at = nrm.at[jz, rows_of(tt)]
        return remote(at, at, agy_s.at[0], agy_r.at[0], tp=tp_at(1 - y, c))

    def ag_f(p, tt):
        at = nrm.at[1 - jz, rows_of(tt, p)]
        return remote(at, at, agf_s.at[p], agf_r.at[p], tp=tp_at(1 - y, c))

    def ag_c(k, cc):
        j, tt = ((jz, tp_at(y, cc)), (jz, tp_at(1 - y, cc)),
                 (1 - jz, tp_at(y, cc)), (1 - jz, tp_at(1 - y, cc)))[k]
        at = nrm.at[j, rows_of(tt)]
        return remote(at, at, agc_s.at[k], agc_r.at[k], tp=tp_at(y, 1 - c))

    go(None, [P(ag_z, 0, jz), P(ag_y, tp), P(ag_z, 1, jz), P(ag_c, 0, c)])

    relay(None, gu_in(3, my_h), gu_over(3))

    for p in range(2):
        got(None, [P(ag_z, p, 1 - jz)])
        go(None, [P(ag_f, p, tp)])
    go(None, [P(ag_c, 2, c)])
    got(None, [P(ag_y, tp_at(1 - y, c))])
    go(None, [P(ag_c, 1, c)])

    def gate_up(j, col, zi):
        side = (1 - col) * x + col * (1 - x)
        columns = pl.ds(pl.multiple_of((2 * zi + side) * chunk, chunk), chunk)
        weights = gux[zi] if col else gub[zi, my_h]
        acc[j] += jnp.dot(nrm[j, :, columns], weights, preferred_element_type=F32)

    def gu_crossed(zi):
        for p in everyp:
            cut = pl.ds(p * gr, gr)
            remote(
                gub.at[zi, my_h, cut], gux.at[zi, cut],
                gux_s.at[zi, p], gux_r.at[zi, p], sp=2 * z + 1 - x,
            ).wait_recv()

    acc[...] = jnp.zeros_like(acc)
    got(None, [P(ag_c, 0, 1 - c), P(ag_c, 1, 1 - c)])
    relay(inner, dn_in(2, h_end), dn_to(2, h_end, 0, 1))
    relay(inner, dn_in(3, h_end), dn_to(3, h_end, 0, 1))
    relay(end, dn_in(1, my_h), dn_over(twin))

    def near_rows(k, carry):
        zi = rank(k)
        gate_up(jz, 0, zi)
        gu_crossed(zi)
        gate_up(jz, 1, zi)
        return carry

    def other_rows(k, carry):
        zi = rank(k)
        gate_up(1 - jz, 0, zi)
        gate_up(1 - jz, 1, zi)
        return carry

    lax.fori_loop(0, 2, near_rows, 0)
    for p in range(2):
        got(None, [P(ag_f, p, tp_at(1 - y, c))])
    go(None, [P(ag_c, 3, c)])
    lax.fori_loop(2, 3, near_rows, 0)
    got(None, [P(ag_c, 2, 1 - c), P(ag_c, 3, 1 - c)])
    relay(inner, dn_in(2, my_h), dn_over(2))
    lax.fori_loop(0, 3, other_rows, 0)
    last = mz(3)
    gate_up(jz, 0, last)
    gate_up(1 - jz, 0, last)
    gu_crossed(last)
    gate_up(jz, 1, last)
    gate_up(1 - jz, 1, last)

    def edge_x():
        return remote(eg_out, eg_x, eg_s.at[0], eg_r.at[0], sp=2 * z + 1 - x)

    def edge_p():
        return remote(eg_out, eg_p, eg_s.at[1], eg_r.at[1], sp=2 * far + 1 - x)

    rim = [acc[j, at:at + 1, :] for j in range(2) for at in (0, rows - 1)]
    rim.append(jnp.zeros((eg_out.shape[0] - 4, 2 * ff), F32))
    eg_out[...] = jnp.concatenate(rim, axis=0).astype(BF16)
    go(None, [edge_x])
    go(cross == 1, [edge_p])

    @pl.when(cross == 0)
    def _():
        eg_p[...] = jnp.zeros_like(eg_p)

    relay(end, dn_in(2, my_h), dn_over(2))

    def convolved(j, lane, taps_ref, start, count, low, high):
        cut = slice(lane, lane + ff)
        now = acc[j, start:start + count, cut].astype(BF16).astype(F32)
        line = lax.broadcasted_iota(jnp.int32, now.shape, 0)
        before = pltpu.roll(now, 1, 0)
        after = pltpu.roll(now, count - 1, 0)
        before = jnp.where(line == 0, 0.0 if low is None else low[:, cut], before)
        after = jnp.where(line == count - 1, 0.0 if high is None else high[:, cut], after)
        taps = taps_ref[:, pl.ds(pl.multiple_of(my_h * ff, ff), ff)]
        return before * taps[0:1] + now * taps[1:2] + after * taps[2:3]

    def gated(j, start, count, low=None, high=None):
        gate = convolved(j, 0, cg_ref, start, count, low, high)
        up = convolved(j, ff, cu_ref, start, count, low, high)
        return (gate / (1.0 + jnp.exp(-gate)) * up).astype(BF16)

    for j in range(2):
        out = gated(j, 0, rows)
        for yy in range(2):
            for cc in range(2):
                at = tp_at(yy, cc) * own
                to = (j * 2 + yy) * own
                hid[cc, to:to + own, :] = out[at:at + own]

    got(None, [edge_x])
    got(cross == 1, [edge_p])

    is_right = x == 1
    beside, beyond = eg_x[...].astype(F32), eg_p[...].astype(F32)
    lows = (jnp.where(is_right, beside[1:2], beyond[3:4]), jnp.where(is_right, beside[3:4], beside[1:2]))
    highs = (jnp.where(is_right, beside[2:3], beside[0:1]), jnp.where(is_right, beyond[0:1], beside[2:3]))
    tile, slab = 16, 32
    for j in range(2):
        first = gated(j, 0, slab, low=lows[j])
        hid[0, 2 * j * own:2 * j * own + tile, :] = first[:tile]
        final = gated(j, rows - slab, slab, high=highs[j])
        stop = (2 * j + 2) * own
        hid[1, stop - tile:stop, :] = final[slab - tile:]

    def d1_copy(b):
        return remote(p2.at[b], s2a.at[b], d1_s.at[b], d1_r.at[b], tp=tp_at(y, 1 - c))

    def d2_copy(b, k):
        jj, yy = ((jz, 1 - y), (1 - jz, y), (1 - jz, 1 - y))[k]
        where = ({"tp": tp_at(1 - y, c)}, {"sp": 2 * mate + x},
                 {"sp": 2 * mate + x, "tp": tp_at(1 - y, c)})[k]
        return remote(
            q2.at[b, 2 * jj + yy], s2b.at[b, k], d2_s.at[b, k], d2_r.at[b, k], **where
        )

    def block_of(col, vb):
        side = (1 - col) * x + col * (1 - x)
        return 2 * mz(vb) + side

    def first_sum(col, vb):
        b = block_of(col, vb)
        weights = dnx[mz(vb)] if col else dnb[mz(vb), my_h]
        p2[b] = jnp.dot(hid[1 - c], weights, preferred_element_type=F32).astype(BF16)
        go(None, [P(d1_copy, b)])
        own2[b] = jnp.dot(hid[c], weights, preferred_element_type=F32)

    def second_sum(col, vb):
        b = block_of(col, vb)
        got(None, [P(d1_copy, b)])
        value = own2[b] + s2a[b].astype(F32)
        own2[b] = value
        short = value.astype(BF16)
        for k in range(4):
            q2[b, k] = short[k * own:(k + 1) * own]
        go(None, [P(d2_copy, b, k) for k in (2, 0, 1)])

    def down(k):
        first_sum(0, ranks[k])
        got(None, dn_over(ranks[k]))
        first_sum(1, ranks[k])

    def pass_on(k):
        second_sum(0, ranks[k])
        second_sum(1, ranks[k])

    def last_over(cond):
        relay(cond, dn_in(3, my_h), dn_over(3))

    last_over(inner)
    down(0)
    down(1)
    pass_on(0)
    last_over(end)
    down(2)
    pass_on(1)
    pass_on(2)
    down(3)
    pass_on(3)

    dcols = dnx.shape[2]
    here = pl.ds(pl.multiple_of((2 * jz + y) * own, own), own)

    for b in range(own2.shape[0]):
        got(None, [P(d2_copy, b, i) for i in range(3)])
        cut = slice(b * dcols, (b + 1) * dcols)
        value = own2[b, here, :]
        for i in range(3):
            value = value + s2b[b, i].astype(F32)
        out_ref[:, cut] = (mid[:, cut] + value).astype(out_ref.dtype)

    for cond, copies in sent:
        def run(copies=copies):
            for copy in copies:
                copy().wait_send()
        under(cond, run)


def on_device(n, tp_n, *args):
    (x_res, q_a, k_a, v_a, q_b, k_b, v_b, gain_qa, gain_ka, gain_qb, gain_kb, w_out_a, w_out_b,
     gain_mid, w_gate, w_up, conv_gate, conv_up, w_down) = args
    ff = w_gate.shape[1] // 2
    chunk, dcols = w_gate.shape[0], w_down.shape[1]
    if n != 8 or tp_n != 4 or chunk % 128 or dcols % 128 or w_gate.shape[1] % 256 or (
        k_a.shape[1] != DHA or k_b.shape[1] != DHB
    ):
        return on_device_narrow(*args)
    rows = q_a.shape[0]
    own, width = x_res.shape
    heads_a, heads_b = q_a.shape[1] // DHA, q_b.shape[1] // DHB
    freq_a, freq_b = lane_frequencies(DHA, 2 * DHA), lane_frequencies(DHB, DHB)
    vmem = pl.BlockSpec(memory_space=pltpu.VMEM)
    hbm = pl.BlockSpec(memory_space=pltpu.MemorySpace.HBM)
    kv_width = 2 * k_a.shape[1] + 2 * k_b.shape[1]
    dma = pltpu.SemaphoreType.DMA
    scratch = [
        pltpu.VMEM((2, 4, rows, kv_width), BF16),
        pltpu.VMEM((heads_a, rows, 2 * DHA), BF16),
        pltpu.VMEM((heads_b, rows, DHB), BF16),
        pltpu.VMEM((heads_a, rows, 128), F32),
        pltpu.VMEM((heads_a, rows, 2 * DHA), F32),
        pltpu.VMEM((heads_b, rows, 128), F32),
        pltpu.VMEM((heads_b, rows, 2 * DHB), F32),
        pltpu.VMEM(w_out_a.shape, BF16),
        pltpu.VMEM(w_out_b.shape, BF16),
        pltpu.VMEM((4, 2, chunk, 2 * ff), BF16),
        pltpu.VMEM((4, chunk, 2 * ff), BF16),
        pltpu.VMEM((4, 2, ff, dcols), BF16),
        pltpu.VMEM((4, ff, dcols), BF16),
        pltpu.VMEM((rows, q_a.shape[1] + q_b.shape[1]), BF16),
        pltpu.VMEM((2, own, width), BF16),
        pltpu.VMEM((2, own, width), F32),
        pltpu.VMEM((2, own, width), BF16),
        pltpu.VMEM((own, width), BF16),
        pltpu.VMEM((own, width), BF16),
        pltpu.VMEM((own, width), F32),
        pltpu.VMEM((2, rows, width), BF16),
        pltpu.VMEM((2, rows, 2 * ff), F32),
        pltpu.VMEM((16, 2 * ff), BF16),
        pltpu.VMEM((16, 2 * ff), BF16),
        pltpu.VMEM((16, 2 * ff), BF16),
        pltpu.VMEM((2, rows, ff), BF16),
        pltpu.VMEM((n, rows, dcols), BF16),
        pltpu.VMEM((n, rows, dcols), F32),
        pltpu.VMEM((n, rows, dcols), BF16),
        pltpu.VMEM((n, 4, own, dcols), BF16),
        pltpu.VMEM((n, 3, own, dcols), BF16),
        dma((8,)),
        dma((2, 4)), dma((4,)), dma((4,)), dma((4,)),
        dma((2, 4, 2, GU_PIECES)), dma((4, 2, GU_PIECES)), dma((4, GU_PIECES)), dma((4, GU_PIECES)),
        dma((2, 4, 2, DN_PIECES)), dma((4, 2, DN_PIECES)), dma((4, DN_PIECES)), dma((4, DN_PIECES)),
        dma((2,)), dma((2,)), dma((1,)), dma((1,)),
        dma((2,)), dma((2,)), dma((1,)), dma((1,)), dma((2,)), dma((2,)), dma((4,)), dma((4,)),
        dma((2,)), dma((2,)),
        dma((n,)), dma((n,)), dma((n, 3)), dma((n, 3)),
    ]
    return pl.pallas_call(
        kernel,
        out_shape=jax.ShapeDtypeStruct(x_res.shape, BF16),
        in_specs=[vmem] * 13 + [hbm, hbm, vmem, hbm, hbm, vmem, vmem, hbm],
        out_specs=vmem,
        scratch_shapes=scratch,
        compiler_params=pltpu.CompilerParams(
            collective_id=0, has_side_effects=True, vmem_limit_bytes=60 * 1024 * 1024
        ),
        name="layer",
    )(
        x_res, q_a, jnp.transpose(k_a), jnp.transpose(v_a), q_b, k_b, v_b,
        gain_qa[None], gain_ka[None], gain_qb[None], gain_kb[None],
        freq_a, freq_b,
        w_out_a, w_out_b, gain_mid[None], w_gate, w_up, conv_gate, conv_up, w_down,
    )


def extended(block, sides, width):
    for axis, dim in sides:
        count = lax.axis_size(axis)
        forward = [(i, i + 1) for i in range(count - 1)]
        backward = [(target, source) for source, target in forward]
        low = lax.ppermute(
            lax.slice_in_dim(block, block.shape[dim] - width, None, axis=dim), axis, forward
        )
        high = lax.ppermute(lax.slice_in_dim(block, 0, width, axis=dim), axis, backward)
        block = jnp.concatenate([low, block, high], axis=dim)
    return block


def rotate_half(values):
    first, second = jnp.split(values, 2, axis=-1)
    return jnp.concatenate([-second, first], axis=-1)


def prepare(raw, gain, head_size, positions):
    count = raw.shape[0]
    heads = raw.shape[1] // head_size
    values = raw.astype(jnp.float32).reshape(count, heads, head_size)
    values = values * lax.rsqrt(jnp.mean(values * values, axis=-1, keepdims=True) + norm_eps)
    values = values * gain
    angles = rotary_angles(positions, head_size)
    cosine, sine = jnp.cos(angles), jnp.sin(angles)
    row_part, col_part = jnp.split(values, 2, axis=-1)
    turned = jnp.concatenate([rotate_half(row_part), rotate_half(col_part)], axis=-1)
    values = values * cosine[:, None, :] + turned * sine[:, None, :]
    return values.astype(jnp.bfloat16)


def start_state(queries):
    count, kv_heads, groups, head_size = queries.shape
    lowest = jnp.full((kv_heads, groups, count), -1e30, jnp.float32)
    totals = jnp.zeros((kv_heads, groups, count), jnp.float32)
    summed = jnp.zeros((kv_heads, groups, count, head_size), jnp.float32)
    return (lowest, totals, summed)


def attend(state, queries, key_piece, value_piece):
    head_size = queries.shape[3]
    kv_heads = queries.shape[1]
    length = key_piece.shape[0]
    keys = key_piece.reshape(length, kv_heads, head_size)
    values = value_piece.reshape(length, kv_heads, head_size)
    span = length
    while span > 1024 and span % 2 == 0:
        span = span // 2
    scale = jnp.float32(head_size ** (-0.5))

    def one_span(index, carry):
        running, totals, summed = carry
        key_rows = lax.dynamic_slice_in_dim(keys, index * span, span, 0)
        value_rows = lax.dynamic_slice_in_dim(values, index * span, span, 0)
        scores = (
            jnp.einsum("qkgd,skd->kgqs", queries, key_rows, preferred_element_type=jnp.float32)
            * scale
        )
        highest = jnp.maximum(running, jnp.max(scores, axis=-1))
        factor = jnp.exp(running - highest)
        expd = jnp.exp(scores - highest[..., None])
        totals = totals * factor + jnp.sum(expd, axis=-1)
        summed = summed * factor[..., None] + jnp.einsum(
            "kgqs,skd->kgqd",
            expd.astype(jnp.bfloat16),
            value_rows,
            preferred_element_type=jnp.float32,
        )
        return (highest, totals, summed)

    return lax.fori_loop(0, length // span, one_span, state)


def finish(state):
    running, totals, summed = state
    kv_heads, groups, count, head_size = summed.shape
    result = summed / totals[..., None]
    return (
        jnp.transpose(result, (2, 0, 1, 3))
        .reshape(count, kv_heads * groups * head_size)
        .astype(jnp.bfloat16)
    )


def on_device_narrow(
    x_res,
    q_a,
    k_a,
    v_a,
    q_b,
    k_b,
    v_b,
    gain_qa,
    gain_ka,
    gain_qb,
    gain_kb,
    w_out_a,
    w_out_b,
    gain_mid,
    w_gate,
    w_up,
    conv_gate,
    conv_up,
    w_down,
):
    tok_rows = q_a.shape[0]
    whole_gate, whole_up, whole_down = (
        lax.all_gather(w_gate, "sp", axis=0, tiled=True),
        lax.all_gather(w_up, "sp", axis=0, tiled=True),
        lax.all_gather(w_down, "sp", axis=1, tiled=True),
    )
    positions = lax.axis_index("sp") * tok_rows + lax.iota(jnp.int32, tok_rows)
    kv_a = k_a.shape[1] // DHA
    kv_b = k_b.shape[1] // DHB
    query_a = prepare(q_a, gain_qa, DHA, positions)
    query_a = query_a.reshape(tok_rows, kv_a, query_a.shape[1] // kv_a, DHA)
    query_b = prepare(q_b, gain_qb, DHB, positions)
    query_b = query_b.reshape(tok_rows, kv_b, query_b.shape[1] // kv_b, DHB)
    keys_a = prepare(k_a, gain_ka, DHA, positions).reshape(tok_rows, kv_a * DHA)
    keys_b = prepare(k_b, gain_kb, DHB, positions).reshape(tok_rows, kv_b * DHB)
    state_a = attend(
        start_state(query_a),
        query_a,
        lax.all_gather(keys_a, "sp", axis=0, tiled=True),
        lax.all_gather(v_a, "sp", axis=0, tiled=True),
    )
    state_b = attend(
        start_state(query_b),
        query_b,
        lax.all_gather(keys_b, "sp", axis=0, tiled=True),
        lax.all_gather(v_b, "sp", axis=0, tiled=True),
    )
    attn_a = finish(state_a)
    attn_b = finish(state_b)
    projected = lax.psum_scatter(
        (
            jnp.dot(attn_a, w_out_a, preferred_element_type=jnp.float32)
            + jnp.dot(attn_b, w_out_b, preferred_element_type=jnp.float32)
        ).astype(jnp.bfloat16),
        "tp",
        scatter_dimension=0,
        tiled=True,
    ).astype(jnp.float32)
    middle = x_res.astype(jnp.float32) + projected
    normed = middle * lax.rsqrt(jnp.mean(middle * middle, axis=-1, keepdims=True) + norm_eps)
    normed = (normed * gain_mid).astype(jnp.bfloat16)
    gathered = lax.all_gather(normed, "tp", axis=0, tiled=True)
    gate_pre = jnp.dot(gathered, whole_gate, preferred_element_type=jnp.float32)
    up_pre = jnp.dot(gathered, whole_up, preferred_element_type=jnp.float32)
    width = gate_pre.shape[1]
    joined = jnp.concatenate([gate_pre, up_pre], axis=1).astype(jnp.bfloat16)
    padded = extended(joined, (("sp", 0),), 1)
    taps = jnp.concatenate([conv_gate, conv_up], axis=1)
    mixed = padded[:-2] * taps[0] + padded[1:-1] * taps[1] + padded[2:] * taps[2]
    hidden = (jax.nn.silu(mixed[:, :width]) * mixed[:, width:]).astype(jnp.bfloat16)
    terms = jnp.dot(hidden, whole_down, preferred_element_type=jnp.float32)
    summed = lax.psum_scatter(
        terms.astype(jnp.bfloat16), "tp", scatter_dimension=0, tiled=True
    ).astype(jnp.float32)
    return (middle + summed).astype(jnp.bfloat16)


def solution(mesh):
    in_specs = (
        P(("sp", "tp"), None),
        P("sp", "tp"),
        P("sp", "tp"),
        P("sp", "tp"),
        P("sp", "tp"),
        P("sp", "tp"),
        P("sp", "tp"),
        P(),
        P(),
        P(),
        P(),
        P("tp", None),
        P("tp", None),
        P(),
        P("sp", "tp"),
        P("sp", "tp"),
        P(None, "tp"),
        P(None, "tp"),
        P("tp", "sp"),
    )
    out_specs = P(("sp", "tp"), None)
    body = functools.partial(on_device, mesh.shape["sp"], mesh.shape["tp"])
    return jax.shard_map(
        body, mesh=mesh, in_specs=in_specs, out_specs=out_specs, check_vma=False
    )
```

```python
import functools

import jax
import jax.numpy as jnp
import numpy as np
from jax import lax
from jax.experimental import pallas as pl
from jax.experimental.pallas import tpu as pltpu
from jax.sharding import PartitionSpec as P

DHA = 64
DHB = 128

norm_eps = 1e-06
rope_theta = 10000.0
F32 = jnp.float32
BF16 = jnp.bfloat16
MESH = pl.DeviceIdType.MESH
GU_PIECES = 4
DN_PIECES = 2
LOG2E = 1.4426950408889634
PAIRED = True
TAIL = 1


def rotary_angles(positions, head_size):
    half = head_size // 2
    inverse = jnp.power(jnp.float32(rope_theta), -jnp.arange(0, half, 2, dtype=jnp.float32) / half)
    grid_row = (positions // 64).astype(jnp.float32)[:, None] * inverse[None, :]
    grid_col = (positions % 64).astype(jnp.float32)[:, None] * inverse[None, :]
    return jnp.concatenate([grid_row, grid_row, grid_col, grid_col], axis=-1)


def lane_frequencies(head_size, width):
    half = head_size // 2
    steps = -np.arange(0, half, 2, dtype=np.float32) / np.float32(half)
    inverse = np.power(np.float32(rope_theta), steps).astype(np.float32)
    return jnp.asarray(np.tile(inverse, width // inverse.shape[0])[None])


def block_mean(width, head):
    i = lax.broadcasted_iota(jnp.int32, (width, width), 0)
    j = lax.broadcasted_iota(jnp.int32, (width, width), 1)
    return jnp.where(lax.div(i, head) == lax.div(j, head), F32(1.0 / head), F32(0.0))


def block_turn(width, head):
    quarter = head // 4
    i = lax.broadcasted_iota(jnp.int32, (width, width), 0)
    j = lax.broadcasted_iota(jnp.int32, (width, width), 1)
    first = lax.rem(j, 2 * quarter) < quarter
    return jnp.where(
        first & (i == j + quarter),
        F32(-1.0),
        jnp.where(jnp.logical_not(first) & (i == j - quarter), F32(1.0), F32(0.0)),
    )


def exact_dot(a, b):
    return jnp.dot(a, b, precision=lax.Precision.HIGHEST, preferred_element_type=F32)


def prepared(raw, gain, angle_cos, angle_sin, head):
    width = raw.shape[1]
    values = raw.astype(F32)
    values = values * lax.rsqrt(exact_dot(values * values, block_mean(width, head)) + norm_eps)
    values = values * gain
    turned = exact_dot(values, block_turn(width, head))
    return (values * angle_cos + turned * angle_sin).astype(BF16)


def kernel(
    x_in, qa_in, kat_in, vat_in, qb_in, kb_in, vb_in,
    gqa_in, gka_in, gqb_in, gkb_in,
    fra_in, frb_in,
    woa_hbm, wob_hbm, gmid_in, wg_hbm, wu_hbm, cg_in, cu_in, wd_hbm,
    out_ref,
    x_ref, qa_ref, kat_ref, vat_ref, qb_ref, kb_ref, vb_ref,
    gqa_ref, gka_ref, gqb_ref, gkb_ref, fra_ref, frb_ref, gmid_ref, cg_ref, cu_ref,
    kv, qas, qbs, m_a, acc_a, m_b, acc_b,
    woa, wob, gub, gux, dnb, dnx,
    attn, pout, own1, s1_in, q1, s2_in, mid, nrm, acc, eg_out, eg_x, eg_p, hid,
    p2, own2, s2a, q2, s2b,
    loc_sem, in_sem, kvz_s, kvz_r, kvx_s, kvx_r, guz_s, guz_r, gux_s, gux_r,
    dnz_s, dnz_r, dnx_s, dnx_r, s1_s, s1_r, s2_s, s2_r,
    agz_s, agz_r, agy_s, agy_r, agf_s, agf_r, agc_s, agc_r, eg_s, eg_r,
    d1_s, d1_r, d2_s, d2_r,
):
    sp = lax.axis_index("sp")
    tp = lax.axis_index("tp")
    z, x = lax.div(sp, 2), lax.rem(sp, 2)
    y, c = lax.div(tp, 2), lax.rem(tp, 2)
    rows = qa_ref.shape[0]
    own = x_ref.shape[0]
    chunk, ff = gub.shape[2], gub.shape[3] // 2
    flip = lax.div(z, 2)

    def mz(v):
        return (1 - flip) * v + flip * (3 - v)

    u = mz(z)
    inner, end = u == 1, u == 0
    mate = mz(1 - u)
    my_h = lax.rem(z, 2)
    jz = my_h
    h_end, h_in = lax.rem(mz(0), 2), lax.rem(mz(1), 2)
    cross = lax.rem(x + flip, 2)
    far = 2 * (1 - flip) * 2 - 2 + z
    twin = 1 - u
    ranks = [u, twin, 2, 3]

    def tp_at(yy, cc):
        return yy * 2 + cc

    barrier = pltpu.get_barrier_semaphore()
    greet = [
        (None, {"sp": 2 * z + 1 - x}),
        (None, {"tp": tp_at(y, 1 - c)}),
        (None, {"tp": tp_at(1 - y, c)}),
        (None, {"sp": 2 * mate + x}),
        (None, {"sp": 2 * mate + x, "tp": tp_at(1 - y, c)}),
        (inner, {"sp": 2 * mz(2) + x}),
        (cross == 1, {"sp": 2 * far + 1 - x}),
    ]
    for cond, where in greet:
        def signal(where=where):
            pl.semaphore_signal(barrier, inc=1, device_id=where, device_id_type=MESH)
        if cond is None:
            signal()
        else:
            pl.when(cond)(signal)

    staged = (
        (kat_in, kat_ref), (vat_in, vat_ref), (kb_in, kb_ref), (vb_in, vb_ref),
        (gka_in, gka_ref), (gkb_in, gkb_ref), (fra_in, fra_ref), (frb_in, frb_ref),
        (qa_in, qa_ref), (qb_in, qb_ref), (gqa_in, gqa_ref), (gqb_in, gqb_ref),
        (x_in, x_ref), (gmid_in, gmid_ref), (cg_in, cg_ref), (cu_in, cu_ref),
    )
    moves = [
        pltpu.make_async_copy(src, dst, in_sem.at[k]) for k, (src, dst) in enumerate(staged)
    ]
    for copy in moves[:8]:
        copy.start()

    loc = []
    for h in range(2):
        cut = pl.ds(h * ff, ff)
        loc.append(pltpu.make_async_copy(
            wg_hbm.at[:, cut], gub.at[z, h, :, pl.ds(0, ff)], loc_sem.at[len(loc)]))
        loc.append(pltpu.make_async_copy(
            wu_hbm.at[:, cut], gub.at[z, h, :, pl.ds(ff, ff)], loc_sem.at[len(loc)]))
    for h in range(2):
        loc.append(pltpu.make_async_copy(
            wd_hbm.at[pl.ds(h * ff, ff)], dnb.at[z, h], loc_sem.at[len(loc)]))
    loc.append(pltpu.make_async_copy(woa_hbm, woa, loc_sem.at[len(loc)]))
    loc.append(pltpu.make_async_copy(wob_hbm, wob, loc_sem.at[len(loc)]))
    for copy in loc[:4] + moves[8:12] + loc[4:] + moves[12:]:
        copy.start()

    def remote(src, dst, send, recv, **where):
        return pltpu.make_async_remote_copy(
            src_ref=src, dst_ref=dst, send_sem=send, recv_sem=recv,
            device_id=where, device_id_type=MESH,
        )

    sent = []

    def under(cond, run):
        if cond is None:
            run()
        else:
            pl.when(cond)(run)

    def go(cond, copies):
        def run():
            for copy in copies:
                copy().start()
        under(cond, run)
        sent.append((cond, copies))

    def got(cond, copies):
        def run():
            for copy in copies:
                copy().wait_recv()
        under(cond, run)

    def relay(cond, arriving, *leaving):
        def run():
            for k, copy in enumerate(arriving):
                copy().wait_recv()
                for copies in leaving:
                    copies[k]().start()
        under(cond, run)
        for copies in leaving:
            sent.append((cond, copies))

    P = functools.partial
    gr, dr = chunk // GU_PIECES, ff // DN_PIECES
    everyp, everyd = range(GU_PIECES), range(DN_PIECES)

    def kv_z(vb, to, way):
        zi = mz(vb)
        return remote(kv.at[0, zi], kv.at[0, zi], kvz_s.at[way, zi], kvz_r.at[zi], sp=2 * mz(to) + x)

    def kv_x(vb):
        zi = mz(vb)
        return remote(kv.at[0, zi], kv.at[1, zi], kvx_s.at[zi], kvx_r.at[zi], sp=2 * z + 1 - x)

    def gu_z(vb, h, p, to, way):
        zi, cut = mz(vb), pl.ds(p * gr, gr)
        return remote(
            gub.at[zi, h, cut], gub.at[zi, h, cut],
            guz_s.at[way, zi, h, p], guz_r.at[zi, h, p], sp=2 * mz(to) + x,
        )

    def gu_x(vb, p):
        zi, cut = mz(vb), pl.ds(p * gr, gr)
        return remote(
            gub.at[zi, my_h, cut], gux.at[zi, cut],
            gux_s.at[zi, p], gux_r.at[zi, p], sp=2 * z + 1 - x,
        )

    def dn_z(vb, h, p, to, way):
        zi, cut = mz(vb), pl.ds(p * dr, dr)
        return remote(
            dnb.at[zi, h, cut], dnb.at[zi, h, cut],
            dnz_s.at[way, zi, h, p], dnz_r.at[zi, h, p], sp=2 * mz(to) + x,
        )

    def dn_x(vb, p):
        zi, cut = mz(vb), pl.ds(p * dr, dr)
        return remote(
            dnb.at[zi, my_h, cut], dnx.at[zi, cut],
            dnx_s.at[zi, p], dnx_r.at[zi, p], sp=2 * z + 1 - x,
        )

    def gu_to(vb, h, to, way, pieces=everyp):
        return [P(gu_z, vb, h, p, to, way) for p in pieces]

    def dn_to(vb, h, to, way):
        return [P(dn_z, vb, h, p, to, way) for p in everyd]

    def gu_over(vb, pieces=everyp):
        return [P(gu_x, vb, p) for p in pieces]

    def dn_over(vb):
        return [P(dn_x, vb, p) for p in everyd]

    def gu_in(vb, h):
        return [P(gu_z, vb, h, p, 1 - u, 0) for p in everyp]

    def dn_in(vb, h):
        return [P(dn_z, vb, h, p, 1 - u, 0) for p in everyd]

    def kv_in(vb):
        return [P(kv_z, vb, 1 - u, 0)]

    for copy in loc[:4]:
        copy.wait()
    pl.semaphore_wait(barrier, 5 + u + cross)
    go(inner, gu_to(u, h_in, 2, 0, [0, 1]))
    go(inner, gu_to(u, h_end, 0, 1, [0, 1]))
    go(end, gu_to(u, h_in, 1, 0, [0]))
    go(None, gu_over(u, [0, 1]))

    def tables(freq_ref, head):
        shape = (rows, freq_ref.shape[1])
        token = lax.broadcasted_iota(jnp.int32, shape, 0) + sp * rows
        lane = lax.broadcasted_iota(jnp.int32, shape, 1)
        grid = jnp.where(lax.rem(lane, head) < head // 2, lax.div(token, 64), lax.rem(token, 64))
        angles = grid.astype(F32) * freq_ref[...]
        return jnp.cos(angles), jnp.sin(angles)

    for copy in moves[:8]:
        copy.wait()
    ca, sa = tables(fra_ref, DHA)
    cb, sb = tables(frb_ref, DHB)
    wka, wkb = kat_ref.shape[0], kb_ref.shape[1]

    def wide(table, width):
        if width <= table.shape[1]:
            return table[:, :width]
        return jnp.concatenate([table] * (width // table.shape[1]), axis=1)

    def gains(ref, width):
        g = ref[...]
        count = width // g.shape[1]
        return g if count == 1 else jnp.concatenate([g] * count, axis=1)

    raw_a = jnp.transpose(kat_ref[...].astype(F32))
    val_a = jnp.transpose(vat_ref[...].astype(F32)).astype(BF16)
    keys_a = prepared(raw_a, gains(gka_ref, wka), wide(ca, wka), wide(sa, wka), DHA)
    keys_b = prepared(kb_ref[...], gains(gkb_ref, wkb), wide(cb, wkb), wide(sb, wkb), DHB)
    kv[0, z, :, :wkb] = keys_b
    kv[0, z, :, wkb:2 * wkb] = vb_ref[...]
    kv[0, z, :, 2 * wkb:] = jnp.concatenate([keys_a, val_a], axis=1)

    go(inner, [P(kv_z, u, 2, 0), P(kv_z, u, 0, 1)])
    go(end, [P(kv_z, u, 1, 0)])
    go(None, [P(kv_x, u)])
    go(end, gu_to(u, h_in, 1, 0, everyp[1:]) + gu_to(u, h_end, 1, 0))
    for copy in loc[4:] + moves[8:]:
        copy.wait()
    go(end, dn_to(u, h_in, 1, 0) + dn_to(u, h_end, 1, 0))

    heads_a = qa_ref.shape[1] // DHA
    heads_b = qb_ref.shape[1] // DHB
    qa = prepared(
        qa_ref[...], gains(gqa_ref, heads_a * DHA), wide(ca, heads_a * DHA),
        wide(sa, heads_a * DHA), DHA,
    )
    qb = prepared(
        qb_ref[...], gains(gqb_ref, heads_b * DHB), wide(cb, heads_b * DHB),
        wide(sb, heads_b * DHB), DHB,
    )
    for h in range(heads_a):
        qas[h] = jnp.concatenate([qa[:, h * DHA:(h + 1) * DHA], jnp.zeros((rows, wka), BF16)], axis=1)
    for h in range(heads_b):
        qbs[h] = qb[:, h * DHB:(h + 1) * DHB]
    for ref, low in ((m_a, -1e30), (m_b, -1e30), (acc_a, 0.0), (acc_b, 0.0)):
        ref[...] = jnp.full(ref.shape, low, F32)

    def attend_one(query, keys, values, head, m, total, h):
        scale = F32(head ** (-0.5) * LOG2E)
        scores = [
            lax.dot_general(
                query, key, (((1,), (1,)), ((), ())), preferred_element_type=F32
            ) * scale
            for key in keys
        ]
        most = functools.reduce(jnp.maximum, scores)
        before = m[h]
        highest = jnp.maximum(before, jnp.max(most, axis=-1, keepdims=True))
        factor = jnp.exp2(before - highest)
        level = wide_to(highest, most.shape[1])
        added = functools.reduce(jnp.add, [
            jnp.dot(jnp.exp2(score - level).astype(BF16), value, preferred_element_type=F32)
            for score, value in zip(scores, values)
        ])
        total[h] = total[h] * wide_to(factor, added.shape[1]) + added
        m[h] = highest

    def wide_to(table, width):
        return jnp.concatenate([table] * (width // table.shape[1]), axis=1)

    ones_b = jnp.ones((rows, wkb), BF16)
    is_key = lax.broadcasted_iota(jnp.int32, (rows, 2 * wka), 1) < wka

    def attend(*blocks):
        keys = [kv[col, zi, :, :wkb] for col, zi in blocks]
        values = [
            jnp.concatenate([kv[col, zi, :, wkb:2 * wkb], ones_b], axis=1) for col, zi in blocks
        ]
        for h in range(heads_b):
            attend_one(qbs[h], keys, values, DHB, m_b, acc_b, h)
        keys = [kv[col, zi, :, 2 * wkb:] for col, zi in blocks]
        values = [jnp.where(is_key, BF16(1.0), pair) for pair in keys]
        for h in range(heads_a):
            attend_one(qas[h], keys, values, DHA, m_a, acc_a, h)

    def rank(k):
        high = k // 2 if isinstance(k, int) else lax.div(k, 2)
        return mz(high * k + (1 - high) * (k + u - 2 * k * u))

    attend((0, z))

    def kv_crossed(zi):
        remote(
            kv.at[0, zi], kv.at[1, zi], kvx_s.at[zi], kvx_r.at[zi], sp=2 * z + 1 - x
        ).wait_recv()

    def attend_step(i, carry):
        @pl.when(i == 1)
        def _():
            got(None, kv_in(twin))
            go(inner, [P(kv_z, 0, 2, 0)])
            go(None, [P(kv_x, twin)])
            got(inner, kv_in(2))
            go(inner, [P(kv_z, 2, 0, 1), P(kv_x, 2)])
            go(inner, gu_to(u, h_in, 2, 0, everyp[2:]) + gu_to(u, h_end, 0, 1, [2]))
            go(end, gu_over(u, [2]))

        @pl.when(i == 2)
        def _():
            got(end, kv_in(2))
            go(end, [P(kv_x, 2)])
            got(inner, kv_in(3))
            go(inner, [P(kv_z, 3, 0, 1), P(kv_x, 3)])
            go(inner, gu_to(u, h_end, 0, 1, everyp[3:]) + gu_over(u, [2]))
            go(None, gu_over(u, everyp[3:]))
            relay(inner, gu_in(0, h_in), gu_to(0, h_in, 2, 0), gu_over(twin))
            go(inner, gu_to(u, h_end, 2, 0))

        @pl.when(i == 3)
        def _():
            got(end, kv_in(3))
            go(end, [P(kv_x, 3)])
            relay(inner, gu_in(2, h_end), gu_to(2, h_end, 0, 1))

        if not PAIRED:
            attend((0, rank(i)))

        @pl.when(i == 3)
        def _():
            relay(end, gu_in(1, my_h), gu_over(twin))
            relay(inner, gu_in(0, h_end), gu_to(0, h_end, 2, 0))
            go(inner, dn_to(u, h_in, 2, 0))

        back = rank(i - 1)
        kv_crossed(back)
        if PAIRED:
            attend((0, rank(i)), (1, back))
        else:
            attend((1, back))
        return carry

    lax.fori_loop(1, 4, attend_step, 0)
    kv_crossed(rank(3))
    attend((1, rank(3)))

    relay(inner, gu_in(3, h_end), gu_to(3, h_end, 0, 1))
    got(inner, dn_in(0, h_in))
    go(inner, dn_to(0, h_in, 2, 0) + dn_to(u, h_end, 2, 0))
    go(None, dn_over(u))

    for h in range(heads_a):
        both = acc_a[h]
        attn[:, h * DHA:(h + 1) * DHA] = (both[:, wka:] / both[:, :wka]).astype(BF16)
    width_a = heads_a * DHA
    for h in range(heads_b):
        attn[:, width_a + h * DHB:width_a + (h + 1) * DHB] = (
            acc_b[h, :, :wkb] / acc_b[h, :, wkb:]
        ).astype(BF16)

    def s1_copy(k):
        yy = (1 - y, y)[k]
        return remote(
            pout.at[yy], s1_in.at[yy], s1_s.at[k], s1_r.at[k], tp=tp_at(y, 1 - c)
        )

    def s2_copy():
        return remote(q1, s2_in, s2_s.at[0], s2_r.at[0], tp=tp_at(1 - y, c))

    for who, cc in enumerate((1 - c, c)):
        for k, yy in enumerate((1 - y, y)):
            block = attn[pl.ds(pl.multiple_of(tp_at(yy, cc) * own, own), own), :]
            value = (
                jnp.dot(block[:, :width_a], woa[...], preferred_element_type=F32)
                + jnp.dot(block[:, width_a:], wob[...], preferred_element_type=F32)
            )
            if who == 0:
                pout[yy] = value.astype(BF16)
                go(None, [P(s1_copy, k)])
            else:
                own1[yy] = value

    got(None, [P(s1_copy, 0)])
    q1[...] = (own1[1 - y] + s1_in[1 - y].astype(F32)).astype(BF16)
    go(None, [s2_copy])

    relay(None, gu_in(2, my_h), gu_over(2))
    got(inner, dn_in(0, h_end))
    go(inner, dn_to(0, h_end, 2, 0) + dn_to(u, h_end, 0, 1) + dn_over(twin))

    mine = pl.ds(pl.multiple_of(tp * own, own), own)
    got(None, [P(s1_copy, 1)])
    middle = x_ref[...].astype(F32) + own1[y] + s1_in[y].astype(F32)
    got(None, [s2_copy])
    middle = middle + s2_in[...].astype(F32)
    mid[...] = middle
    normed = middle * lax.rsqrt(jnp.mean(middle * middle, axis=-1, keepdims=True) + norm_eps)
    nrm[jz, mine, :] = (normed * gmid_ref[...]).astype(BF16)

    part = own // 2

    def rows_of(tt, p=None):
        if p is None:
            return pl.ds(pl.multiple_of(tt * own, own), own)
        return pl.ds(pl.multiple_of(tt * own + p * part, part), part)

    def ag_z(p, j):
        at = nrm.at[j, rows_of(tp, p)]
        return remote(at, at, agz_s.at[p], agz_r.at[p], sp=2 * mate + x)

    def ag_y(tt):
        at = nrm.at[jz, rows_of(tt)]
        return remote(at, at, agy_s.at[0], agy_r.at[0], tp=tp_at(1 - y, c))

    def ag_f(p, tt):
        at = nrm.at[1 - jz, rows_of(tt, p)]
        return remote(at, at, agf_s.at[p], agf_r.at[p], tp=tp_at(1 - y, c))

    def ag_c(k, cc):
        j, tt = ((jz, tp_at(y, cc)), (jz, tp_at(1 - y, cc)),
                 (1 - jz, tp_at(y, cc)), (1 - jz, tp_at(1 - y, cc)))[k]
        at = nrm.at[j, rows_of(tt)]
        return remote(at, at, agc_s.at[k], agc_r.at[k], tp=tp_at(y, 1 - c))

    go(None, [P(ag_z, 0, jz), P(ag_y, tp), P(ag_z, 1, jz), P(ag_c, 0, c)])

    relay(None, gu_in(3, my_h), gu_over(3))

    for p in range(2):
        got(None, [P(ag_z, p, 1 - jz)])
        go(None, [P(ag_f, p, tp)])
    go(None, [P(ag_c, 2, c)])
    got(None, [P(ag_y, tp_at(1 - y, c))])
    go(None, [P(ag_c, 1, c)])

    def gate_up(j, col, zi):
        side = (1 - col) * x + col * (1 - x)
        columns = pl.ds(pl.multiple_of((2 * zi + side) * chunk, chunk), chunk)
        weights = gux[zi] if col else gub[zi, my_h]
        acc[j] += jnp.dot(nrm[j, :, columns], weights, preferred_element_type=F32)

    def gu_crossed(zi):
        for p in everyp:
            cut = pl.ds(p * gr, gr)
            remote(
                gub.at[zi, my_h, cut], gux.at[zi, cut],
                gux_s.at[zi, p], gux_r.at[zi, p], sp=2 * z + 1 - x,
            ).wait_recv()

    acc[...] = jnp.zeros_like(acc)
    got(None, [P(ag_c, 0, 1 - c), P(ag_c, 1, 1 - c)])
    relay(inner, dn_in(2, h_end), dn_to(2, h_end, 0, 1))
    relay(inner, dn_in(3, h_end), dn_to(3, h_end, 0, 1))
    relay(end, dn_in(1, my_h), dn_over(twin))

    def near_rows(k, carry):
        zi = rank(k)
        gate_up(jz, 0, zi)
        gu_crossed(zi)
        gate_up(jz, 1, zi)
        return carry

    def other_rows(k, carry):
        zi = rank(k)
        gate_up(1 - jz, 0, zi)
        gate_up(1 - jz, 1, zi)
        return carry

    lax.fori_loop(0, 2, near_rows, 0)
    for p in range(2):
        got(None, [P(ag_f, p, tp_at(1 - y, c))])
    go(None, [P(ag_c, 3, c)])
    lax.fori_loop(2, 3, near_rows, 0)
    got(None, [P(ag_c, 2, 1 - c), P(ag_c, 3, 1 - c)])
    relay(inner, dn_in(2, my_h), dn_over(2))
    lax.fori_loop(0, 3, other_rows, 0)
    last = mz(3)
    gate_up(jz, 0, last)
    gate_up(1 - jz, 0, last)
    gu_crossed(last)
    gate_up(jz, 1, last)
    gate_up(1 - jz, 1, last)

    def edge_x():
        return remote(eg_out, eg_x, eg_s.at[0], eg_r.at[0], sp=2 * z + 1 - x)

    def edge_p():
        return remote(eg_out, eg_p, eg_s.at[1], eg_r.at[1], sp=2 * far + 1 - x)

    rim = [acc[j, at:at + 1, :] for j in range(2) for at in (0, rows - 1)]
    rim.append(jnp.zeros((eg_out.shape[0] - 4, 2 * ff), F32))
    eg_out[...] = jnp.concatenate(rim, axis=0).astype(BF16)
    go(None, [edge_x])
    go(cross == 1, [edge_p])

    @pl.when(cross == 0)
    def _():
        eg_p[...] = jnp.zeros_like(eg_p)

    relay(end, dn_in(2, my_h), dn_over(2))

    def convolved(j, lane, taps_ref, start, count, low, high):
        cut = slice(lane, lane + ff)
        now = acc[j, start:start + count, cut].astype(BF16).astype(F32)
        line = lax.broadcasted_iota(jnp.int32, now.shape, 0)
        before = pltpu.roll(now, 1, 0)
        after = pltpu.roll(now, count - 1, 0)
        before = jnp.where(line == 0, 0.0 if low is None else low[:, cut], before)
        after = jnp.where(line == count - 1, 0.0 if high is None else high[:, cut], after)
        taps = taps_ref[:, pl.ds(pl.multiple_of(my_h * ff, ff), ff)]
        return before * taps[0:1] + now * taps[1:2] + after * taps[2:3]

    def gated(j, start, count, low=None, high=None):
        gate = convolved(j, 0, cg_ref, start, count, low, high)
        up = convolved(j, ff, cu_ref, start, count, low, high)
        return (gate / (1.0 + jnp.exp(-gate)) * up).astype(BF16)

    for j in range(2):
        out = gated(j, 0, rows)
        for yy in range(2):
            for cc in range(2):
                at = tp_at(yy, cc) * own
                to = (j * 2 + yy) * own
                hid[cc, to:to + own, :] = out[at:at + own]

    got(None, [edge_x])
    got(cross == 1, [edge_p])

    is_right = x == 1
    beside, beyond = eg_x[...].astype(F32), eg_p[...].astype(F32)
    lows = (jnp.where(is_right, beside[1:2], beyond[3:4]), jnp.where(is_right, beside[3:4], beside[1:2]))
    highs = (jnp.where(is_right, beside[2:3], beside[0:1]), jnp.where(is_right, beyond[0:1], beside[2:3]))
    tile, slab = 16, 32
    for j in range(2):
        first = gated(j, 0, slab, low=lows[j])
        hid[0, 2 * j * own:2 * j * own + tile, :] = first[:tile]
        final = gated(j, rows - slab, slab, high=highs[j])
        stop = (2 * j + 2) * own
        hid[1, stop - tile:stop, :] = final[slab - tile:]

    def d1_copy(b):
        return remote(p2.at[b], s2a.at[b], d1_s.at[b], d1_r.at[b], tp=tp_at(y, 1 - c))

    def d2_copy(b, k):
        jj, yy = ((jz, 1 - y), (1 - jz, y), (1 - jz, 1 - y))[k]
        where = ({"tp": tp_at(1 - y, c)}, {"sp": 2 * mate + x},
                 {"sp": 2 * mate + x, "tp": tp_at(1 - y, c)})[k]
        return remote(
            q2.at[b, 2 * jj + yy], s2b.at[b, k], d2_s.at[b, k], d2_r.at[b, k], **where
        )

    def block_of(col, vb):
        side = (1 - col) * x + col * (1 - x)
        return 2 * mz(vb) + side

    def first_sum(col, vb):
        b = block_of(col, vb)
        weights = dnx[mz(vb)] if col else dnb[mz(vb), my_h]
        p2[b] = jnp.dot(hid[1 - c], weights, preferred_element_type=F32).astype(BF16)
        go(None, [P(d1_copy, b)])
        own2[b] = jnp.dot(hid[c], weights, preferred_element_type=F32)

    def second_sum(col, vb):
        b = block_of(col, vb)
        got(None, [P(d1_copy, b)])
        value = own2[b] + s2a[b].astype(F32)
        own2[b] = value
        short = value.astype(BF16)
        for k in range(4):
            q2[b, k] = short[k * own:(k + 1) * own]
        go(None, [P(d2_copy, b, k) for k in (2, 0, 1)])

    def down(k):
        first_sum(0, ranks[k])
        got(None, dn_over(ranks[k]))
        first_sum(1, ranks[k])

    def pass_on(k):
        second_sum(0, ranks[k])
        second_sum(1, ranks[k])

    def last_over(cond):
        relay(cond, dn_in(3, my_h), dn_over(3))

    last_over(inner)
    down(0)
    down(1)
    pass_on(0)
    last_over(end)
    down(2)
    pass_on(1)
    pass_on(2)
    down(3)
    pass_on(3)

    dcols = dnx.shape[2]
    here = pl.ds(pl.multiple_of((2 * jz + y) * own, own), own)

    for cond, copies in sent:
        def run(copies=copies):
            for copy in copies:
                copy().wait_send()
        under(cond, run)

    for b in range(own2.shape[0]):
        got(None, [P(d2_copy, b, i) for i in range(3)])
        cut = slice(b * dcols, (b + 1) * dcols)
        value = own2[b, here, :]
        for i in range(3):
            value = value + s2b[b, i].astype(F32)
        out_ref[:, cut] = (mid[:, cut] + value).astype(out_ref.dtype)


def on_device(n, tp_n, *args):
    (x_res, q_a, k_a, v_a, q_b, k_b, v_b, gain_qa, gain_ka, gain_qb, gain_kb, w_out_a, w_out_b,
     gain_mid, w_gate, w_up, conv_gate, conv_up, w_down) = args
    ff = w_gate.shape[1] // 2
    chunk, dcols = w_gate.shape[0], w_down.shape[1]
    if n != 8 or tp_n != 4 or chunk % 128 or dcols % 128 or w_gate.shape[1] % 256 or (
        k_a.shape[1] != DHA or k_b.shape[1] != DHB
    ):
        return on_device_narrow(*args)
    rows = q_a.shape[0]
    own, width = x_res.shape
    heads_a, heads_b = q_a.shape[1] // DHA, q_b.shape[1] // DHB
    freq_a, freq_b = lane_frequencies(DHA, 2 * DHA), lane_frequencies(DHB, DHB)
    vmem = pl.BlockSpec(memory_space=pltpu.VMEM)
    hbm = pl.BlockSpec(memory_space=pltpu.MemorySpace.HBM)
    kv_width = 2 * k_a.shape[1] + 2 * k_b.shape[1]
    dma = pltpu.SemaphoreType.DMA
    scratch = [
        pltpu.VMEM((2, 4, rows, kv_width), BF16),
        pltpu.VMEM((heads_a, rows, 2 * DHA), BF16),
        pltpu.VMEM((heads_b, rows, DHB), BF16),
        pltpu.VMEM((heads_a, rows, 128), F32),
        pltpu.VMEM((heads_a, rows, 2 * DHA), F32),
        pltpu.VMEM((heads_b, rows, 128), F32),
        pltpu.VMEM((heads_b, rows, 2 * DHB), F32),
        pltpu.VMEM(w_out_a.shape, BF16),
        pltpu.VMEM(w_out_b.shape, BF16),
        pltpu.VMEM((4, 2, chunk, 2 * ff), BF16),
        pltpu.VMEM((4, chunk, 2 * ff), BF16),
        pltpu.VMEM((4, 2, ff, dcols), BF16),
        pltpu.VMEM((4, ff, dcols), BF16),
        pltpu.VMEM((rows, q_a.shape[1] + q_b.shape[1]), BF16),
        pltpu.VMEM((2, own, width), BF16),
        pltpu.VMEM((2, own, width), F32),
        pltpu.VMEM((2, own, width), BF16),
        pltpu.VMEM((own, width), BF16),
        pltpu.VMEM((own, width), BF16),
        pltpu.VMEM((own, width), F32),
        pltpu.VMEM((2, rows, width), BF16),
        pltpu.VMEM((2, rows, 2 * ff), F32),
        pltpu.VMEM((16, 2 * ff), BF16),
        pltpu.VMEM((16, 2 * ff), BF16),
        pltpu.VMEM((16, 2 * ff), BF16),
        pltpu.VMEM((2, rows, ff), BF16),
        pltpu.VMEM((n, rows, dcols), BF16),
        pltpu.VMEM((n, rows, dcols), F32),
        pltpu.VMEM((n, rows, dcols), BF16),
        pltpu.VMEM((n, 4, own, dcols), BF16),
        pltpu.VMEM((n, 3, own, dcols), BF16),
        dma((8,)), dma((16,)),
        dma((2, 4)), dma((4,)), dma((4,)), dma((4,)),
        dma((2, 4, 2, GU_PIECES)), dma((4, 2, GU_PIECES)), dma((4, GU_PIECES)), dma((4, GU_PIECES)),
        dma((2, 4, 2, DN_PIECES)), dma((4, 2, DN_PIECES)), dma((4, DN_PIECES)), dma((4, DN_PIECES)),
        dma((2,)), dma((2,)), dma((1,)), dma((1,)),
        dma((2,)), dma((2,)), dma((1,)), dma((1,)), dma((2,)), dma((2,)), dma((4,)), dma((4,)),
        dma((2,)), dma((2,)),
        dma((n,)), dma((n,)), dma((n, 3)), dma((n, 3)),
    ]
    operands = (
        x_res, q_a, jnp.transpose(k_a), jnp.transpose(v_a), q_b, k_b, v_b,
        gain_qa[None], gain_ka[None], gain_qb[None], gain_kb[None],
        freq_a, freq_b,
        w_out_a, w_out_b, gain_mid[None], w_gate, w_up, conv_gate, conv_up, w_down,
    )
    small = operands[:13] + (operands[15],) + operands[18:20]
    scratch = [pltpu.VMEM(a.shape, a.dtype) for a in small] + scratch
    return pl.pallas_call(
        kernel,
        out_shape=jax.ShapeDtypeStruct(x_res.shape, BF16),
        in_specs=[hbm] * len(operands),
        out_specs=vmem,
        scratch_shapes=scratch,
        compiler_params=pltpu.CompilerParams(
            collective_id=0, has_side_effects=True, vmem_limit_bytes=60 * 1024 * 1024
        ),
        name="layer",
    )(*operands)


def extended(block, sides, width):
    for axis, dim in sides:
        count = lax.axis_size(axis)
        forward = [(i, i + 1) for i in range(count - 1)]
        backward = [(target, source) for source, target in forward]
        low = lax.ppermute(
            lax.slice_in_dim(block, block.shape[dim] - width, None, axis=dim), axis, forward
        )
        high = lax.ppermute(lax.slice_in_dim(block, 0, width, axis=dim), axis, backward)
        block = jnp.concatenate([low, block, high], axis=dim)
    return block


def rotate_half(values):
    first, second = jnp.split(values, 2, axis=-1)
    return jnp.concatenate([-second, first], axis=-1)


def prepare(raw, gain, head_size, positions):
    count = raw.shape[0]
    heads = raw.shape[1] // head_size
    values = raw.astype(jnp.float32).reshape(count, heads, head_size)
    values = values * lax.rsqrt(jnp.mean(values * values, axis=-1, keepdims=True) + norm_eps)
    values = values * gain
    angles = rotary_angles(positions, head_size)
    cosine, sine = jnp.cos(angles), jnp.sin(angles)
    row_part, col_part = jnp.split(values, 2, axis=-1)
    turned = jnp.concatenate([rotate_half(row_part), rotate_half(col_part)], axis=-1)
    values = values * cosine[:, None, :] + turned * sine[:, None, :]
    return values.astype(jnp.bfloat16)


def start_state(queries):
    count, kv_heads, groups, head_size = queries.shape
    lowest = jnp.full((kv_heads, groups, count), -1e30, jnp.float32)
    totals = jnp.zeros((kv_heads, groups, count), jnp.float32)
    summed = jnp.zeros((kv_heads, groups, count, head_size), jnp.float32)
    return (lowest, totals, summed)


def attend(state, queries, key_piece, value_piece):
    head_size = queries.shape[3]
    kv_heads = queries.shape[1]
    length = key_piece.shape[0]
    keys = key_piece.reshape(length, kv_heads, head_size)
    values = value_piece.reshape(length, kv_heads, head_size)
    span = length
    while span > 1024 and span % 2 == 0:
        span = span // 2
    scale = jnp.float32(head_size ** (-0.5))

    def one_span(index, carry):
        running, totals, summed = carry
        key_rows = lax.dynamic_slice_in_dim(keys, index * span, span, 0)
        value_rows = lax.dynamic_slice_in_dim(values, index * span, span, 0)
        scores = (
            jnp.einsum("qkgd,skd->kgqs", queries, key_rows, preferred_element_type=jnp.float32)
            * scale
        )
        highest = jnp.maximum(running, jnp.max(scores, axis=-1))
        factor = jnp.exp(running - highest)
        expd = jnp.exp(scores - highest[..., None])
        totals = totals * factor + jnp.sum(expd, axis=-1)
        summed = summed * factor[..., None] + jnp.einsum(
            "kgqs,skd->kgqd",
            expd.astype(jnp.bfloat16),
            value_rows,
            preferred_element_type=jnp.float32,
        )
        return (highest, totals, summed)

    return lax.fori_loop(0, length // span, one_span, state)


def finish(state):
    running, totals, summed = state
    kv_heads, groups, count, head_size = summed.shape
    result = summed / totals[..., None]
    return (
        jnp.transpose(result, (2, 0, 1, 3))
        .reshape(count, kv_heads * groups * head_size)
        .astype(jnp.bfloat16)
    )


def on_device_narrow(
    x_res,
    q_a,
    k_a,
    v_a,
    q_b,
    k_b,
    v_b,
    gain_qa,
    gain_ka,
    gain_qb,
    gain_kb,
    w_out_a,
    w_out_b,
    gain_mid,
    w_gate,
    w_up,
    conv_gate,
    conv_up,
    w_down,
):
    tok_rows = q_a.shape[0]
    whole_gate, whole_up, whole_down = (
        lax.all_gather(w_gate, "sp", axis=0, tiled=True),
        lax.all_gather(w_up, "sp", axis=0, tiled=True),
        lax.all_gather(w_down, "sp", axis=1, tiled=True),
    )
    positions = lax.axis_index("sp") * tok_rows + lax.iota(jnp.int32, tok_rows)
    kv_a = k_a.shape[1] // DHA
    kv_b = k_b.shape[1] // DHB
    query_a = prepare(q_a, gain_qa, DHA, positions)
    query_a = query_a.reshape(tok_rows, kv_a, query_a.shape[1] // kv_a, DHA)
    query_b = prepare(q_b, gain_qb, DHB, positions)
    query_b = query_b.reshape(tok_rows, kv_b, query_b.shape[1] // kv_b, DHB)
    keys_a = prepare(k_a, gain_ka, DHA, positions).reshape(tok_rows, kv_a * DHA)
    keys_b = prepare(k_b, gain_kb, DHB, positions).reshape(tok_rows, kv_b * DHB)
    state_a = attend(
        start_state(query_a),
        query_a,
        lax.all_gather(keys_a, "sp", axis=0, tiled=True),
        lax.all_gather(v_a, "sp", axis=0, tiled=True),
    )
    state_b = attend(
        start_state(query_b),
        query_b,
        lax.all_gather(keys_b, "sp", axis=0, tiled=True),
        lax.all_gather(v_b, "sp", axis=0, tiled=True),
    )
    attn_a = finish(state_a)
    attn_b = finish(state_b)
    projected = lax.psum_scatter(
        (
            jnp.dot(attn_a, w_out_a, preferred_element_type=jnp.float32)
            + jnp.dot(attn_b, w_out_b, preferred_element_type=jnp.float32)
        ).astype(jnp.bfloat16),
        "tp",
        scatter_dimension=0,
        tiled=True,
    ).astype(jnp.float32)
    middle = x_res.astype(jnp.float32) + projected
    normed = middle * lax.rsqrt(jnp.mean(middle * middle, axis=-1, keepdims=True) + norm_eps)
    normed = (normed * gain_mid).astype(jnp.bfloat16)
    gathered = lax.all_gather(normed, "tp", axis=0, tiled=True)
    gate_pre = jnp.dot(gathered, whole_gate, preferred_element_type=jnp.float32)
    up_pre = jnp.dot(gathered, whole_up, preferred_element_type=jnp.float32)
    width = gate_pre.shape[1]
    joined = jnp.concatenate([gate_pre, up_pre], axis=1).astype(jnp.bfloat16)
    padded = extended(joined, (("sp", 0),), 1)
    taps = jnp.concatenate([conv_gate, conv_up], axis=1)
    mixed = padded[:-2] * taps[0] + padded[1:-1] * taps[1] + padded[2:] * taps[2]
    hidden = (jax.nn.silu(mixed[:, :width]) * mixed[:, width:]).astype(jnp.bfloat16)
    terms = jnp.dot(hidden, whole_down, preferred_element_type=jnp.float32)
    summed = lax.psum_scatter(
        terms.astype(jnp.bfloat16), "tp", scatter_dimension=0, tiled=True
    ).astype(jnp.float32)
    return (middle + summed).astype(jnp.bfloat16)


def solution(mesh):
    in_specs = (
        P(("sp", "tp"), None),
        P("sp", "tp"),
        P("sp", "tp"),
        P("sp", "tp"),
        P("sp", "tp"),
        P("sp", "tp"),
        P("sp", "tp"),
        P(),
        P(),
        P(),
        P(),
        P("tp", None),
        P("tp", None),
        P(),
        P("sp", "tp"),
        P("sp", "tp"),
        P(None, "tp"),
        P(None, "tp"),
        P("tp", "sp"),
    )
    out_specs = P(("sp", "tp"), None)
    body = functools.partial(on_device, mesh.shape["sp"], mesh.shape["tp"])
    return jax.shard_map(
        body, mesh=mesh, in_specs=in_specs, out_specs=out_specs, check_vma=False
    )
```
